512 devices in a mesh: sp: 64 (over z, y), fs: 4 (over x), tp: 2 (over core).
Axes of the slice: x: 4, y: 8, z: 8, core: 2. Of those that a mesh axis runs over, the one named last changes fastest.
Arguments:
- tokens: bfloat16 [65536, 2048], P(('fs', 'sp')), parts along dimension 0, may hold values from -6 to 6
- norm_gain: float32 [2048], replicated, may hold values from 0.1 to 1.9
- w_query: bfloat16 [2048, 1024], P('sp', 'tp'), may hold values from -0.080939698 to 0.080939698
- w_key: bfloat16 [2048, 256], P('sp', 'tp'), may hold values from -0.080939698 to 0.080939698
- w_value: bfloat16 [2048, 256], P('sp', 'tp'), may hold values from -0.125 to 0.125
- w_conv_in: bfloat16 [2048, 1024], P('sp', 'tp'), may hold values from -0.125 to 0.125
- w_conv_gate: bfloat16 [2048, 1024], P('sp', 'tp'), may hold values from -0.125 to 0.125
- sink_logit: float32 [16], P('tp'), may hold values from 2 to 6
- conv_taps: float32 [31, 1024], P(None, 'tp'), may hold values from -5.3881591 to 5.3881591
- conv_bias: float32 [1024], P('tp'), may hold values from -0.9 to 5.9
- channel_gain: float32 [1024], P('tp'), may hold values from 0.1 to 1.9
- channel_shift: float32 [1024], P('tp'), may hold values from -3 to 3
- w_attn_out: bfloat16 [1024, 2048], P(None, 'sp'), may hold values from -1.5 to 1.5
- w_conv_out: bfloat16 [1024, 2048], P(None, 'sp'), may hold values from -0.1875 to 0.1875
Outputs:
- output: bfloat16 [65536, 2048], P(('fs', 'sp', 'tp')), parts along dimension 0
The draws below stay inside these ranges and needn't reach their ends.
There are 4 independent parts, one for each index of `fs`. The reference program is written for one: setup_inputs(seed, part) draws one part's arguments, and reference() takes and returns one part's arrays. A program takes and returns all parts, laid end to end along the dimension named above; an argument that names none is the same for every part. Nothing has to cross between parts.
All inputs are finite; a program needn't handle non-finite values.
Results may differ from the reference program's by a relative error of at most 0.011.
Values may be sent and summed in bfloat16 or wider, within the bound.
A program may use at most 64 MiB of HBM per device.

```python
import jax
import jax.numpy as jnp
from jax import lax

D = 2048
HEADS = 16
KV_HEADS = 4
HEAD_DIM = 64
CHANNELS = 1024
TAPS = 31
WINDOW = 128
GRID_W = 64
TOK_DEV = 256
SEQ = 16384
ATT_WIDTH = 1024
KV_WIDTH = 256


def draw_tokens(key, part):
    noise_key = jax.random.fold_in(key, 0)
    result = jnp.clip(jax.random.normal(noise_key, (SEQ, D), jnp.float32), -6.0, 6.0)
    return result.astype(jnp.bfloat16)


def draw_w_query(key, part):
    base = jnp.clip(jax.random.normal(jax.random.fold_in(key, 11), (D, HEADS * HEAD_DIM), jnp.float32), -3.0, 3.0) * D ** (-0.5)
    return base.astype(jnp.bfloat16)


def draw_w_key(key, part):
    base = jnp.clip(jax.random.normal(jax.random.fold_in(key, 12), (D, KV_HEADS * HEAD_DIM), jnp.float32), -3.0, 3.0) * D ** (-0.5)
    return base.astype(jnp.bfloat16)


def draw_conv_taps(key, part):
    base_key, jitter_key = jax.random.split(jax.random.fold_in(key, 13))
    base = jnp.clip(jax.random.normal(base_key, (TAPS, CHANNELS), jnp.float32), -3.0, 3.0)
    order = jnp.arange(CHANNELS, dtype=jnp.float32) / CHANNELS
    jitter = jnp.clip(jax.random.normal(jitter_key, (CHANNELS,), jnp.float32), -3.0, 3.0)
    exponent = jnp.clip(order + 0.15 * jitter, 0.0, 1.0)
    return (base * TAPS ** (-0.5) * 10.0 ** exponent[None, :]).astype(jnp.float32)


def draw_conv_bias(key, part):
    order = jnp.arange(CHANNELS, dtype=jnp.float32) / CHANNELS
    jitter = jnp.clip(jax.random.normal(jax.random.fold_in(key, 14), (CHANNELS,), jnp.float32), -3.0, 3.0)
    ramp = 3.0 * order
    return (ramp + 0.3 * jitter).astype(jnp.float32)


def levels(rng, shape, pieces, smallest, largest):
    factor_of = 1.0
    for axis_at, shards_of in pieces:
        draws = jax.random.uniform(jax.random.fold_in(jax.random.fold_in(rng, 6), axis_at), (shards_of,), jnp.float32, smallest / len(pieces), largest / len(pieces))
        factor_of = factor_of * jnp.repeat(jnp.exp(draws), shape[axis_at] // shards_of).reshape((-1,) + (1,) * (len(shape) - 1 - axis_at))
    return factor_of


def normal_values(key, shape, deviation, limit, cuts=(), held_as=jnp.bfloat16):
    array = deviation * jax.random.normal(key, shape, jnp.float32)
    if cuts:
        array = array * levels(key, shape, cuts, -0.22, 0.18)
    return jnp.clip(array, -limit, limit).astype(held_as)


def setup_inputs(seed: int = 0, part: int = 0) -> dict:
    arg_keys = jax.random.split(jax.random.key(seed), 15)
    part_keys = jax.random.split(jax.random.fold_in(arg_keys[14], part), 15)
    tokens = draw_tokens(jax.random.fold_in(jax.random.fold_in(arg_keys[14], part), 71), part)
    norm_gain = jnp.clip(1.0 + 0.18 * jax.random.normal(arg_keys[1], (D,), jnp.float32), 0.1, 1.9)
    w_query = draw_w_query(jax.random.fold_in(arg_keys[14], 71), part)
    w_key = draw_w_key(jax.random.fold_in(arg_keys[14], 71), part)
    w_value = normal_values(arg_keys[4], (D, KV_WIDTH), D ** -0.5, 0.125, ((0, 64), (1, 2)))
    w_conv_in = normal_values(arg_keys[5], (D, CHANNELS), D ** -0.5, 0.125, ((0, 64), (1, 2)))
    w_conv_gate = normal_values(arg_keys[6], (D, CHANNELS), D ** -0.5, 0.125, ((0, 64), (1, 2)))
    sink_logit = jnp.clip(2.0 + 4.0 * jax.random.uniform(arg_keys[7], (HEADS,), jnp.float32) ** levels(arg_keys[7], (HEADS,), ((0, 2),), -0.2, 0.2), 2.0, 6.0)
    conv_taps = draw_conv_taps(jax.random.fold_in(arg_keys[14], 71), part)
    conv_bias = draw_conv_bias(jax.random.fold_in(arg_keys[14], 71), part)
    channel_gain = jnp.clip(1.0 + 0.18 * jax.random.normal(arg_keys[10], (CHANNELS,), jnp.float32), 0.1, 1.9)
    channel_shift = normal_values(arg_keys[11], (CHANNELS,), 0.5, 3.0, ((0, 2),), jnp.float32)
    w_attn_out = normal_values(arg_keys[12], (ATT_WIDTH, D), (max(ATT_WIDTH // 64, 1)) ** -0.5, 1.5, ((1, 64),))
    w_conv_out = normal_values(arg_keys[13], (CHANNELS, D), CHANNELS ** -0.5, 0.1875, ((1, 64),))
    return {"tokens": tokens, "norm_gain": norm_gain, "w_query": w_query, "w_key": w_key, "w_value": w_value, "w_conv_in": w_conv_in, "w_conv_gate": w_conv_gate, "sink_logit": sink_logit, "conv_taps": conv_taps, "conv_bias": conv_bias, "channel_gain": channel_gain, "channel_shift": channel_shift, "w_attn_out": w_attn_out, "w_conv_out": w_conv_out}


EPSILON = 1e-06
NEGATIVE = -1e+30
ROPE_BASE = 10000.0

def rotate_pairs(values, positions):
    middle = values.shape[-1] // 2
    inverse = ROPE_BASE ** (-jnp.arange(middle, dtype=jnp.float32) / middle)
    angles = positions.astype(jnp.float32)[:, None] * inverse[None, :]
    cosine = jnp.cos(angles)[:, None, :]
    sine_table = jnp.sin(angles)[:, None, :]
    leading = values[..., :middle]
    trailing = values[..., middle:]
    return jnp.concatenate([leading * cosine - trailing * sine_table, leading * sine_table + trailing * cosine], axis=-1)

def grid_rotate(values, positions):
    middle = values.shape[-1] // 2
    return jnp.concatenate([rotate_pairs(values[..., :middle], positions // GRID_W), rotate_pairs(values[..., middle:], positions % GRID_W)], axis=-1)

def reference(tokens, norm_gain, w_query, w_key, w_value, w_conv_in, w_conv_gate, sink_logit, conv_taps, conv_bias, channel_gain, channel_shift, w_attn_out, w_conv_out):
    total = tokens.shape[0]
    token_float = tokens.astype(jnp.float32)
    normed = (token_float * lax.rsqrt(lax.optimization_barrier(jnp.mean(token_float * token_float, axis=-1, keepdims=True)) + EPSILON) * norm_gain[None, :]).astype(jnp.bfloat16)
    positions = jnp.arange(total, dtype=jnp.int32)
    group = HEADS // KV_HEADS
    query = jnp.dot(normed, w_query, preferred_element_type=jnp.float32).reshape(total, HEADS, HEAD_DIM)
    query = grid_rotate(query, positions).astype(jnp.bfloat16)
    keys = jnp.dot(normed, w_key, preferred_element_type=jnp.float32).reshape(total, KV_HEADS, HEAD_DIM)
    keys = grid_rotate(keys, positions).astype(jnp.bfloat16)
    values = jnp.dot(normed, w_value, preferred_element_type=jnp.float32).astype(jnp.bfloat16)
    values = values.reshape(total, KV_HEADS, HEAD_DIM)
    padded_keys = jnp.pad(keys, ((WINDOW, WINDOW), (0, 0), (0, 0)))
    padded_values = jnp.pad(values, ((WINDOW, WINDOW), (0, 0), (0, 0)))
    block = min(TOK_DEV, 512)
    span = block + 2 * WINDOW
    sinks = sink_logit.astype(jnp.float32).reshape(KV_HEADS, group)[:, :, None, None]

    def attend(block_index):
        start = (block_index * block).astype(jnp.int32)
        queries = lax.dynamic_slice_in_dim(query, start, block, 0).reshape(block, KV_HEADS, group, HEAD_DIM)
        near_keys = lax.dynamic_slice_in_dim(padded_keys, start, span, 0)
        near_values = lax.dynamic_slice_in_dim(padded_values, start, span, 0)
        scores = jnp.einsum('qkgd,skd->kgqs', queries.astype(jnp.float32), near_keys.astype(jnp.float32)) * HEAD_DIM ** (-0.5)
        query_pos = start + jnp.arange(block, dtype=jnp.int32)
        key_pos = start - WINDOW + jnp.arange(span, dtype=jnp.int32)
        valid = (jnp.abs(query_pos[:, None] - key_pos[None, :]) <= WINDOW) & (key_pos[None, :] >= 0) & (key_pos[None, :] < total)
        scores = jnp.where(valid[None, None], scores, NEGATIVE)
        top = jnp.maximum(lax.optimization_barrier(jnp.max(scores, axis=-1, keepdims=True)), sinks)
        raised = jnp.exp(scores - top)
        denominator = lax.optimization_barrier(jnp.sum(raised, axis=-1, keepdims=True)) + jnp.exp(sinks - top)
        probs = (raised / denominator).astype(jnp.bfloat16)
        mixed = jnp.einsum('kgqs,skd->qkgd', probs.astype(jnp.float32), near_values.astype(jnp.float32))
        return mixed.astype(jnp.bfloat16).reshape(block, HEADS * HEAD_DIM)
    attended = lax.map(attend, jnp.arange(total // block, dtype=jnp.int32)).reshape(total, HEADS * HEAD_DIM)
    glu = (jnp.dot(normed, w_conv_in, preferred_element_type=jnp.float32) * jax.nn.sigmoid(jnp.dot(normed, w_conv_gate, preferred_element_type=jnp.float32))).astype(jnp.bfloat16)
    reach = TAPS // 2
    padded_glu = jnp.pad(glu.astype(jnp.float32), ((reach, reach), (0, 0)))
    filtered = jnp.zeros((total, CHANNELS), jnp.float32) + conv_bias[None, :]
    for offset in range(TAPS):
        filtered = filtered + conv_taps[offset][None, :] * padded_glu[offset:offset + total]
    centre = lax.optimization_barrier(jnp.mean(filtered, axis=-1, keepdims=True))
    centred = filtered - centre
    spread = lax.optimization_barrier(jnp.mean(centred * centred, axis=-1, keepdims=True))
    conv_out = jax.nn.silu(centred * lax.rsqrt(spread + EPSILON) * channel_gain[None, :] + channel_shift[None, :]).astype(jnp.bfloat16)
    result = jnp.dot(attended, w_attn_out, preferred_element_type=jnp.float32) + jnp.dot(conv_out, w_conv_out, preferred_element_type=jnp.float32)
    return result.astype(jnp.bfloat16)
```

```python
import functools
import math

import jax
import jax.numpy as jnp
from jax import lax
from jax.experimental import pallas as pl
from jax.experimental.pallas import tpu as pltpu
from jax.sharding import PartitionSpec as P

HEAD_DIM = 64
WINDOW = 128
EPSILON = 1e-06
NEGATIVE = -1e30
ROPE_BASE = 10000.0
TOK = 256
HALF = 128
D = 2048
TAPS = 31
RING = 8
FS = 4
CHUNK = 512
MESH = pl.DeviceIdType.MESH
NT = (((1,), (1,)), ((), ()))
F32 = jnp.float32
BF16 = jnp.bfloat16


def kernel(
    tokens_ref,
    gain_ref,
    wq_ref,
    wk_ref,
    wv_ref,
    wc_ref,
    wg_ref,
    sink_ref,
    taps_ref,
    bias_ref,
    cgain_ref,
    cshift_ref,
    wao_ref,
    wco_ref,
    out_ref,
    tok,
    win,
    wout,
    ctab,
    stab,
    qbuf,
    kvg,
    gext,
    low,
    high,
    sbuf,
    feat,
    raw,
    cvals,
    stat_out,
    stat_in,
    part,
    part_out,
    part_in,
    in_recv,
    in_send_a,
    in_send_b,
    out_recv,
    out_send_a,
    out_send_b,
    tok_recv,
    tok_send,
    tok_fwd,
    tok_pair,
    halo_recv,
    halo_send,
    feat_recv,
    feat_send,
    stat_sem,
    part_recv,
    part_send,
):
    sp = lax.axis_index("sp")
    f = lax.axis_index("fs")
    c = lax.axis_index("tp")
    z, y = sp // RING, sp % RING
    me_a = (1 - c) * y + c * z
    me_b = (1 - c) * z + c * y
    partner = 1 - c

    def sp_of(a, b):
        return (1 - c) * (b * RING + a) + c * (a * RING + b)

    def wrap(v):
        return (v + 2 * RING) % RING

    def fs_of(step):
        return (f + step) % FS

    has_low = sp > 0
    has_high = sp < RING * RING - 1

    barrier = pltpu.get_barrier_semaphore()

    def greet(**where):
        pl.semaphore_signal(barrier, inc=1, device_id=where, device_id_type=MESH)

    for step in range(1, RING):
        greet(sp=sp_of(wrap(me_a + step), me_b))
    greet(sp=sp_of(me_a, wrap(me_b + 1)))
    greet(sp=sp_of(me_a, wrap(me_b - 1)))
    for step in range(1, FS):
        greet(fs=fs_of(step))
    greet(tp=partner)

    greet(sp=(sp + 1) % (RING * RING))
    greet(sp=(sp + RING * RING - 1) % (RING * RING))

    lane32 = lax.broadcasted_iota(jnp.int32, (32, 128), 1)
    mine = pl.multiple_of(sp * 32, 32)
    cols = pl.ds(pl.multiple_of(f * 128, 128), 128)
    upper = f // 2
    wk = wk_ref[...].astype(F32)
    wv = wv_ref[...].astype(F32)
    pick = (lane32 * 0 + upper) > 0
    wk = jnp.where(pick, pltpu.roll(wk, 64, 1), wk)
    wv = jnp.where(pick, wv, pltpu.roll(wv, 64, 1))
    win[pl.ds(mine, 32), 0:128] = wq_ref[:, cols]
    win[pl.ds(mine, 32), 128:256] = jnp.where(lane32 < 64, wk, wv).astype(BF16)
    win[pl.ds(mine, 32), 256:384] = wc_ref[:, cols]
    win[pl.ds(mine, 32), 384:512] = wg_ref[:, cols]

    def norm_rows(start):
        def body(i, carry):
            rows = pl.ds(pl.multiple_of(start + i * 16, 16), 16)
            x = tokens_ref[rows, :].astype(F32)
            scale = lax.rsqrt(jnp.mean(x * x, axis=-1, keepdims=True) + EPSILON)
            tok[f, rows, :] = (x * scale * gain_ref[...]).astype(BF16)
            return carry

        lax.fori_loop(0, HALF // 16, body, 0)

    norm_rows(pl.multiple_of(c * HALF, HALF))

    pl.semaphore_wait(barrier, RING - 1 + 2 + FS - 1 + 1 + 2)

    def tok_rows(half, piece):
        return pl.ds(pl.multiple_of(half * HALF + piece * 64, 64), 64)

    def tok_copy(slot, half, piece, send, **where):
        ref = tok.at[slot, tok_rows(half, piece)]
        return pltpu.make_async_remote_copy(
            src_ref=ref,
            dst_ref=ref,
            send_sem=send,
            recv_sem=tok_recv.at[slot, half, piece],
            device_id=where,
            device_id_type=MESH,
        )

    def tok_first(direction, piece):
        return tok_copy(f, c, piece, tok_send.at[direction, piece], fs=fs_of(1 + 2 * direction))

    def tok_second(direction):
        slot = fs_of(3 - 2 * direction)
        return tok_copy(slot, c, direction, tok_fwd.at[direction], fs=fs_of(1 + 2 * direction))

    def tok_to_pair(slot, piece):
        return tok_copy(slot, c, piece, tok_pair.at[slot, piece], tp=partner)

    for first in range(2):
        for direction in range(2):
            tok_first(direction, (first + direction) % 2).start()

    def slab(buf, index):
        return buf.at[pl.ds(pl.multiple_of(index * 32, 32), 32)]

    def slab_copy(buf, recv, send, index, target):
        ref = slab(buf, index)
        return pltpu.make_async_remote_copy(
            src_ref=ref,
            dst_ref=ref,
            send_sem=send,
            recv_sem=recv.at[index],
            device_id={"sp": target},
            device_id_type=MESH,
        )

    def a_copy(gather, step):
        buf, recv, send_a, _ = gather
        return slab_copy(buf, recv, send_a.at[step], sp, sp_of(wrap(me_a + step), me_b))

    def b_copy(gather, direction, index):
        buf, recv, _, send_b = gather
        target = sp_of(me_a, wrap(me_b + 1 - 2 * direction))
        return slab_copy(buf, recv, send_b.at[direction, index], index, target)

    def near(j):
        odd = j % 2
        dist = (j + 1) // 2
        return wrap(me_a + odd * dist - (1 - odd) * dist)

    def start_gather(gather):
        b_copy(gather, 0, sp).start()
        b_copy(gather, 1, sp).start()

        def body(step, carry):
            a_copy(gather, step).start()
            return carry

        lax.fori_loop(1, RING, body, 0)

    def serve(gather, first, last):
        def body(n, carry):
            s, j = n // RING, n % RING
            a = near(j)

            @pl.when((s == 0) & (j > 0))
            def _():
                index = sp_of(a, me_b)
                b_copy(gather, 0, index).wait_recv()
                b_copy(gather, 0, index).start()
                b_copy(gather, 1, index).start()

            @pl.when((s > 0) & (s < 4))
            def _():
                index = sp_of(a, wrap(me_b - s))
                b_copy(gather, 0, index).wait_recv()

                @pl.when((s < 3) | (j < 4))
                def _():
                    b_copy(gather, 0, index).start()

                index = sp_of(a, wrap(me_b + s))
                b_copy(gather, 1, index).wait_recv()

                @pl.when((s < 3) | (j >= 4))
                def _():
                    b_copy(gather, 1, index).start()

            @pl.when(s == 4)
            def _():
                b_copy(gather, 0, sp_of(a, wrap(me_b + s))).wait_recv()

            return carry

        lax.fori_loop(first, last, body, 0)

    def end_gather(gather):
        def body(step, carry):
            a_copy(gather, step).wait_send()
            return carry

        lax.fori_loop(1, RING, body, 0)

        def body_b(n, carry):
            s, j = n // RING, n % RING
            a = near(j)

            @pl.when((s < 3) | (j < 4))
            def _():
                b_copy(gather, 0, sp_of(a, wrap(me_b - s))).wait_send()

            @pl.when((s < 3) | (j >= 4))
            def _():
                b_copy(gather, 1, sp_of(a, wrap(me_b + s))).wait_send()

            return carry

        lax.fori_loop(0, 4 * RING, body_b, 0)

    gather_in = (win, in_recv, in_send_a, in_send_b)
    gather_out = (wout, out_recv, out_send_a, out_send_b)
    start_gather(gather_in)

    norm_rows(pl.multiple_of(partner * HALF, HALF))
    serve(gather_in, 1, 8)

    eye = (
        lax.broadcasted_iota(jnp.int32, (32, 32), 0) == lax.broadcasted_iota(jnp.int32, (32, 32), 1)
    ).astype(BF16)
    for k in range(FS):
        rows = pl.ds(pl.multiple_of(c * 512 + k * 128, 128), 128)
        for part_at, ref in ((0, wao_ref), (128, wco_ref)):
            turned = lax.dot_general(eye, ref[rows, :], NT, preferred_element_type=F32)
            at = k * 256 + part_at
            wout[pl.ds(mine, 32), at : at + 128] = turned.astype(BF16)

    serve(gather_in, 8, 16)

    lane = lax.broadcasted_iota(jnp.int32, (HALF, 128), 1)
    frequency = jnp.exp((lane % 16).astype(F32) * (-math.log(ROPE_BASE) / 16))
    for k in range(2):
        token = lax.broadcasted_iota(jnp.int32, (HALF, 128), 0) + k * HALF
        place = jnp.where(lane % 64 < 32, sp * 4 + token // 64, token % 64)
        angle = place.astype(F32) * frequency
        ctab[k * HALF : (k + 1) * HALF, :] = jnp.cos(angle)
        sine = jnp.sin(angle)
        stab[k * HALF : (k + 1) * HALF, :] = jnp.where(lane % 32 < 16, -sine, sine)

    @pl.when(sp == 0)
    def _():
        low[...] = jnp.zeros_like(low)

    @pl.when(sp == RING * RING - 1)
    def _():
        high[...] = jnp.zeros_like(high)

    serve(gather_in, 16, 24)

    for direction in range(2):
        slot = fs_of(3 - 2 * direction)
        tok_to_pair(slot, direction).wait_recv()
        tok_second(direction).start()
        tok_to_pair(slot, direction).start()

    serve(gather_in, 24, 32)

    for direction in range(2):
        slot = fs_of(3 - 2 * direction)
        tok_to_pair(slot, 1 - direction).wait_recv()
        tok_to_pair(slot, 1 - direction).start()

    start_gather(gather_out)
    serve(gather_in, 32, 40)

    def halo_copy(i, side):
        at = side * 144
        return pltpu.make_async_remote_copy(
            src_ref=kvg.at[i, at : at + 144],
            dst_ref=(low if side else high).at[i],
            send_sem=halo_send.at[i, side],
            recv_sem=halo_recv.at[i, side],
            device_id={"sp": sp + 2 * side - 1},
            device_id_type=MESH,
        )

    lanes = lax.broadcasted_iota(jnp.int32, (TOK, 128), 1)

    def rotated(x, cosine, sine):
        other = jnp.where(lanes % 32 < 16, pltpu.roll(x, 112, 1), pltpu.roll(x, 16, 1))
        return x * cosine + other * sine

    def project(i):
        slot = fs_of(i)
        acc = jnp.dot(tok[slot], win[...], preferred_element_type=F32)
        cosine, sine = ctab[...], stab[...]
        query = rotated(acc[:, 0:128], cosine, sine).astype(BF16).astype(F32) * HEAD_DIM**-0.5
        qbuf[i, 0] = jnp.where(lanes < 64, query, 0.0).astype(BF16)
        qbuf[i, 1] = jnp.where(lanes < 64, pltpu.roll(query, 64, 1), 0.0).astype(BF16)
        pair = acc[:, 128:256]
        turned = rotated(pair, cosine, sine)
        kvg[i, 16:272] = jnp.where(lanes < 64, turned, pair).astype(BF16)
        glu = (acc[:, 256:384] * jax.nn.sigmoid(acc[:, 384:512])).astype(BF16)
        kvg[i, 0:16] = glu[0:16]
        kvg[i, 272:288] = glu[240:256]
        gext[i, 16:272] = glu.astype(F32)

        @pl.when(has_low)
        def _():
            halo_copy(i, 0).start()

        @pl.when(has_high)
        def _():
            halo_copy(i, 1).start()

    row_at = lax.broadcasted_iota(jnp.int32, (HALF, 256), 0)
    key_at = lax.broadcasted_iota(jnp.int32, (HALF, 256), 1)
    half_row = lax.broadcasted_iota(jnp.int32, (HALF, 128), 0)
    half_key = lax.broadcasted_iota(jnp.int32, (HALF, 128), 1)
    half_lane = half_key
    far = RING * TOK
    own_valid = (key_at - row_at <= WINDOW, key_at >= row_at)
    halo_valid = (
        half_key >= half_row + jnp.where(has_low, 0, far),
        half_key + jnp.where(has_high, 0, far) <= half_row,
    )

    def mix(i):
        @pl.when(has_low)
        def _():
            halo_copy(i, 1).wait_recv()

        @pl.when(has_high)
        def _():
            halo_copy(i, 0).wait_recv()

        own_kv = kvg[i, 16:272]
        own_ones = jnp.where(
            lax.broadcasted_iota(jnp.int32, (TOK, 128), 1) < 64, jnp.ones_like(own_kv), own_kv
        )
        for block in range(2):
            near_kv = low[i, 0:128] if block == 0 else high[i, 16:144]
            near_ones = jnp.where(half_lane < 64, jnp.ones_like(near_kv), near_kv)
            heads = []
            for h in range(2):
                q = qbuf[i, h, block * HALF : (block + 1) * HALF]
                s_own = lax.dot_general(q, own_kv, NT, preferred_element_type=F32)
                s_near = lax.dot_general(q, near_kv, NT, preferred_element_type=F32)
                s_own = jnp.where(own_valid[block], s_own, NEGATIVE)
                s_near = jnp.where(halo_valid[block], s_near, NEGATIVE)
                sink = sink_ref[2 * f + h]
                top = jnp.maximum(
                    jnp.maximum(s_own[:, 0:128], s_own[:, 128:256]), s_near
                )
                top = jnp.maximum(jnp.max(top, axis=-1, keepdims=True), sink)
                p_own = jnp.exp(s_own - top).astype(BF16)
                p_near = jnp.exp(s_near - top).astype(BF16)
                mixed = jnp.dot(p_own, own_ones, preferred_element_type=F32) + jnp.dot(
                    p_near, near_ones, preferred_element_type=F32
                )
                heads.append(mixed / (pltpu.roll(mixed, 64, 1) + jnp.exp(sink - top)))
            joined = jnp.where(half_lane < 64, pltpu.roll(heads[0], 64, 1), heads[1])
            sbuf[i, block * HALF : (block + 1) * HALF, 0:128] = joined.astype(BF16)

        gext[i, 0:16] = low[i, 128:144].astype(F32)
        gext[i, 272:288] = high[i, 0:16].astype(F32)

        for block in range(4):
            total = jnp.zeros((64, 128), F32)
            for k in range(TAPS):
                at = block * 64 + k + 1
                total = total + taps_ref[k : k + 1, cols] * gext[i, at : at + 64]
            sbuf[i, block * 64 : (block + 1) * 64, 128:256] = total.astype(BF16)

    def feat_copy(i):
        return pltpu.make_async_remote_copy(
            src_ref=sbuf.at[i],
            dst_ref=feat.at[f],
            send_sem=feat_send.at[i],
            recv_sem=feat_recv.at[f],
            device_id={"fs": fs_of(i)},
            device_id_type=MESH,
        )

    def wait_pair(slot):
        tok_copy(slot, partner, 0, tok_fwd.at[0], tp=partner).wait_recv()
        tok_copy(slot, partner, 1, tok_fwd.at[0], tp=partner).wait_recv()

    project(0)
    serve(gather_out, 1, 8)
    wait_pair(fs_of(1))
    project(1)
    wait_pair(fs_of(3))
    project(3)
    serve(gather_out, 8, 12)
    mix(0)
    feat[f] = sbuf[0]
    for piece in range(2):
        tok_to_pair(fs_of(2), piece).wait_recv()
        tok_to_pair(fs_of(2), piece).start()
    serve(gather_out, 12, 16)
    wait_pair(fs_of(2))
    project(2)
    mix(1)
    feat_copy(1).start()
    serve(gather_out, 16, 20)
    mix(3)
    feat_copy(3).start()
    serve(gather_out, 20, 24)
    mix(2)
    feat_copy(2).start()
    serve(gather_out, 24, 32)

    def feat_wait(src):
        pltpu.make_async_remote_copy(
            src_ref=sbuf.at[0],
            dst_ref=feat.at[src],
            send_sem=feat_send.at[0],
            recv_sem=feat_recv.at[src],
            device_id={"tp": partner},
            device_id_type=MESH,
        ).wait_recv()

    for i in (1, 3, 2):
        feat_wait(fs_of(i))

    total = jnp.zeros((TOK, 1), F32)
    for k in range(FS):
        values = feat[k, :, 128:256].astype(F32) + bias_ref[:, k * 128 : (k + 1) * 128]
        cvals[:, k * 128 : (k + 1) * 128] = values
        total = total + jnp.sum(values, axis=-1, keepdims=True)
    here = total / 512.0
    around = jnp.zeros((TOK, 1), F32)
    for k in range(FS):
        centred = cvals[:, k * 128 : (k + 1) * 128] - here
        around = around + jnp.sum(centred * centred, axis=-1, keepdims=True)
    stat_out[...] = jnp.where(lanes < 64, here, around)
    stat_copy = pltpu.make_async_remote_copy(
        src_ref=stat_out,
        dst_ref=stat_in,
        send_sem=stat_sem.at[0],
        recv_sem=stat_sem.at[1],
        device_id={"tp": partner},
        device_id_type=MESH,
    )
    stat_copy.start()
    for k in range(FS):
        raw[:, k * 256 : k * 256 + 128] = feat[k, :, 0:128]
    stat_copy.wait_recv()
    there = stat_in[:, 0:1]
    gap = here - there
    centre = 0.5 * (here + there)
    spread = (around + stat_in[:, 64:65] + 256.0 * gap * gap) / 1024.0
    scale = lax.rsqrt(spread + EPSILON)
    for k in range(FS):
        at = slice(k * 128, (k + 1) * 128)
        v = (cvals[:, at] - centre) * scale * cgain_ref[:, at] + cshift_ref[:, at]
        raw[:, k * 256 + 128 : (k + 1) * 256] = (v / (1.0 + jnp.exp(-v))).astype(BF16)

    serve(gather_out, 32, 40)

    def part_copy(n):
        return pltpu.make_async_remote_copy(
            src_ref=part_out.at[n],
            dst_ref=part_in.at[n],
            send_sem=part_send.at[n],
            recv_sem=part_recv.at[n],
            device_id={"tp": partner},
            device_id_type=MESH,
        )

    mine_rows = pl.ds(pl.multiple_of(c * HALF, HALF), HALF)
    other_rows = pl.ds(pl.multiple_of(partner * HALF, HALF), HALF)
    for n in range(D // CHUNK):
        weights = wout[n * CHUNK : (n + 1) * CHUNK, :]
        part_out[n] = lax.dot_general(
            raw[other_rows, :], weights, NT, preferred_element_type=F32
        ).astype(BF16)
        part_copy(n).start()
        part[n] = lax.dot_general(raw[mine_rows, :], weights, NT, preferred_element_type=F32)
    for n in range(D // CHUNK):
        part_copy(n).wait_recv()
        out_ref[:, n * CHUNK : (n + 1) * CHUNK] = (part[n] + part_in[n].astype(F32)).astype(BF16)

    for n in range(D // CHUNK):
        part_copy(n).wait_send()
    stat_copy.wait_send()
    for i in range(1, FS):
        feat_copy(i).wait_send()
    for i in range(FS):

        @pl.when(has_low)
        def _():
            halo_copy(i, 0).wait_send()

        @pl.when(has_high)
        def _():
            halo_copy(i, 1).wait_send()

    for direction in range(2):
        for piece in range(2):
            tok_first(direction, piece).wait_send()
        tok_second(direction).wait_send()
    for i in range(1, FS):
        for piece in range(2):
            tok_to_pair(fs_of(i), piece).wait_send()
    end_gather(gather_in)
    end_gather(gather_out)


def local(
    tokens,
    norm_gain,
    w_query,
    w_key,
    w_value,
    w_conv_in,
    w_conv_gate,
    sink_logit,
    conv_taps,
    conv_bias,
    channel_gain,
    channel_shift,
    w_attn_out,
    w_conv_out,
):
    vmem = pl.BlockSpec(memory_space=pltpu.VMEM)
    smem = pl.BlockSpec(memory_space=pltpu.SMEM)
    dma = pltpu.SemaphoreType.DMA
    return pl.pallas_call(
        kernel,
        out_shape=jax.ShapeDtypeStruct((HALF, D), BF16),
        in_specs=[vmem] * 7 + [smem] + [vmem] * 6,
        out_specs=vmem,
        scratch_shapes=[
            pltpu.VMEM((FS, TOK, D), BF16),
            pltpu.VMEM((D, 512), BF16),
            pltpu.VMEM((D, 1024), BF16),
            pltpu.VMEM((TOK, 128), F32),
            pltpu.VMEM((TOK, 128), F32),
            pltpu.VMEM((FS, 2, TOK, 128), BF16),
            pltpu.VMEM((FS, 288, 128), BF16),
            pltpu.VMEM((FS, 288, 128), F32),
            pltpu.VMEM((FS, 144, 128), BF16),
            pltpu.VMEM((FS, 144, 128), BF16),
            pltpu.VMEM((FS, TOK, 256), BF16),
            pltpu.VMEM((FS, TOK, 256), BF16),
            pltpu.VMEM((TOK, 1024), BF16),
            pltpu.VMEM((TOK, 512), F32),
            pltpu.VMEM((TOK, 128), F32),
            pltpu.VMEM((TOK, 128), F32),
            pltpu.VMEM((D // CHUNK, HALF, CHUNK), F32),
            pltpu.VMEM((D // CHUNK, HALF, CHUNK), BF16),
            pltpu.VMEM((D // CHUNK, HALF, CHUNK), BF16),
            dma((64,)),
            dma((RING,)),
            dma((2, 64)),
            dma((64,)),
            dma((RING,)),
            dma((2, 64)),
            dma((FS, 2, 2)),
            dma((2, 2)),
            dma((2,)),
            dma((FS, 2)),
            dma((FS, 2)),
            dma((FS, 2)),
            dma((FS,)),
            dma((FS,)),
            dma((2,)),
            dma((D // CHUNK,)),
            dma((D // CHUNK,)),
        ],
        compiler_params=pltpu.CompilerParams(
            collective_id=0, has_side_effects=True, vmem_limit_bytes=60 * 1024 * 1024
        ),
        name="fused",
    )(
        tokens,
        norm_gain.reshape(1, -1),
        w_query,
        w_key,
        w_value,
        w_conv_in,
        w_conv_gate,
        sink_logit,
        conv_taps,
        conv_bias.reshape(1, -1),
        channel_gain.reshape(1, -1),
        channel_shift.reshape(1, -1),
        w_attn_out,
        w_conv_out,
    )


def solution(mesh):
    in_specs = (
        P(("fs", "sp"), None),
        P(),
        P("sp", "tp"),
        P("sp", "tp"),
        P("sp", "tp"),
        P("sp", "tp"),
        P("sp", "tp"),
        P("tp"),
        P(None, "tp"),
        P("tp"),
        P("tp"),
        P("tp"),
        P(None, "sp"),
        P(None, "sp"),
    )
    out_specs = P(("fs", "sp", "tp"), None)
    return jax.shard_map(local, mesh=mesh, in_specs=in_specs, out_specs=out_specs, check_vma=False)
```

```python
import functools
import math

import jax
import jax.numpy as jnp
from jax import lax
from jax.experimental import pallas as pl
from jax.experimental.pallas import tpu as pltpu
from jax.sharding import PartitionSpec as P

HEAD_DIM = 64
WINDOW = 128
EPSILON = 1e-06
NEGATIVE = -1e30
ROPE_BASE = 10000.0
TOK = 256
HALF = 128
D = 2048
TAPS = 31
RING = 8
FS = 4
CHUNK = 512
MESH = pl.DeviceIdType.MESH
NT = (((1,), (1,)), ((), ()))
F32 = jnp.float32
BF16 = jnp.bfloat16


def kernel(*refs):
    (
        tokens_hbm,
        gain_hbm,
        wq_hbm,
        wk_hbm,
        wv_hbm,
        wc_hbm,
        wg_hbm,
        sink_hbm,
        taps_hbm,
        bias_hbm,
        cgain_hbm,
        cshift_hbm,
        wao_hbm,
        wco_hbm,
        out_ref,
        tokens_ref,
        gain_ref,
        wq_ref,
        wk_ref,
        wv_ref,
        wc_ref,
        wg_ref,
        sink_ref,
        taps_ref,
        bias_ref,
        cgain_ref,
        cshift_ref,
        wao_ref,
        wco_ref,
        tok,
        win,
        wout,
        ctab,
        stab,
        qbuf,
        kvg,
        gext,
        low,
        high,
        sbuf,
        feat,
        raw,
        cvals,
        stat_out,
        stat_in,
        part,
        part_out,
        part_in,
        load_sem,
        in_recv_a,
        in_recv_b,
        out_recv_a,
        out_recv_b,
        tok_recv,
        halo_recv,
        feat_recv,
        stat_recv,
        part_recv,
        send_sem,
    ) = refs
    in_sent, out_sent, tok_sent, feat_sent, stat_sent, part_sent = (
        send_sem.at[k] for k in range(6)
    )
    halo_sent = (send_sem.at[6], send_sem.at[7])
    sp = lax.axis_index("sp")
    f = lax.axis_index("fs")
    c = lax.axis_index("tp")
    z, y = sp // RING, sp % RING
    me_a = (1 - c) * y + c * z
    me_b = (1 - c) * z + c * y
    partner = 1 - c

    def sp_of(a, b):
        return (1 - c) * (b * RING + a) + c * (a * RING + b)

    def wrap(v):
        return (v + 2 * RING) % RING

    def fs_of(step):
        return (f + step) % FS

    def load(k, src, dst):
        copy = pltpu.make_async_copy(src, dst, load_sem.at[k])
        copy.start()
        return copy

    own_half = pl.ds(pl.multiple_of(c * HALF, HALF), HALF)
    other_half = pl.ds(pl.multiple_of(partner * HALF, HALF), HALF)
    load_weights = [
        load(0, wq_hbm, wq_ref),
        load(1, wk_hbm, wk_ref),
        load(2, wv_hbm, wv_ref),
        load(3, wc_hbm, wc_ref),
        load(4, wg_hbm, wg_ref),
    ]
    load_own = [
        load(5, gain_hbm, gain_ref),
        load(6, tokens_hbm.at[own_half], tokens_ref.at[own_half]),
    ]
    load_other = load(7, tokens_hbm.at[other_half], tokens_ref.at[other_half])
    load_out = [load(8, wao_hbm, wao_ref), load(9, wco_hbm, wco_ref)]
    load_rest = [
        load(10, sink_hbm, sink_ref),
        load(11, taps_hbm, taps_ref),
        load(12, bias_hbm, bias_ref),
        load(13, cgain_hbm, cgain_ref),
        load(14, cshift_hbm, cshift_ref),
    ]

    has_low = sp > 0
    has_high = sp < RING * RING - 1

    barrier = pltpu.get_barrier_semaphore()

    def greet(**where):
        pl.semaphore_signal(barrier, inc=1, device_id=where, device_id_type=MESH)

    for step in range(1, RING):
        greet(sp=sp_of(wrap(me_a + step), me_b))
    greet(sp=sp_of(me_a, wrap(me_b + 1)))
    greet(sp=sp_of(me_a, wrap(me_b - 1)))
    for step in range(1, FS):
        greet(fs=fs_of(step))
    greet(tp=partner)

    greet(sp=(sp + 1) % (RING * RING))
    greet(sp=(sp + RING * RING - 1) % (RING * RING))

    lane32 = lax.broadcasted_iota(jnp.int32, (32, 128), 1)
    mine = pl.multiple_of(sp * 32, 32)
    cols = pl.ds(pl.multiple_of(f * 128, 128), 128)
    upper = f // 2
    for copy in load_weights:
        copy.wait()
    wk = wk_ref[...].astype(F32)
    wv = wv_ref[...].astype(F32)
    pick = (lane32 * 0 + upper) > 0
    wk = jnp.where(pick, pltpu.roll(wk, 64, 1), wk)
    wv = jnp.where(pick, wv, pltpu.roll(wv, 64, 1))
    win[pl.ds(mine, 32), 0:128] = wq_ref[:, cols]
    win[pl.ds(mine, 32), 128:256] = jnp.where(lane32 < 64, wk, wv).astype(BF16)
    win[pl.ds(mine, 32), 256:384] = wc_ref[:, cols]
    win[pl.ds(mine, 32), 384:512] = wg_ref[:, cols]

    def norm_rows(start):
        def body(i, carry):
            rows = pl.ds(pl.multiple_of(start + i * 16, 16), 16)
            x = tokens_ref[rows, :].astype(F32)
            scale = lax.rsqrt(jnp.mean(x * x, axis=-1, keepdims=True) + EPSILON)
            tok[f, rows, :] = (x * scale * gain_ref[...]).astype(BF16)
            return carry

        lax.fori_loop(0, HALF // 16, body, 0)

    for copy in load_own:
        copy.wait()
    norm_rows(pl.multiple_of(c * HALF, HALF))

    pl.semaphore_wait(barrier, RING - 1 + 2 + FS - 1 + 1 + 2)

    def tok_rows(half, piece):
        return pl.ds(pl.multiple_of(half * HALF + piece * 64, 64), 64)

    def tok_copy(slot, half, piece, **where):
        ref = tok.at[slot, tok_rows(half, piece)]
        return pltpu.make_async_remote_copy(
            src_ref=ref,
            dst_ref=ref,
            send_sem=tok_sent,
            recv_sem=tok_recv.at[slot, half, piece],
            device_id=where,
            device_id_type=MESH,
        )

    def tok_first(direction, piece):
        return tok_copy(f, c, piece, fs=fs_of(1 + 2 * direction))

    def tok_second(direction):
        slot = fs_of(3 - 2 * direction)
        return tok_copy(slot, c, direction, fs=fs_of(1 + 2 * direction))

    def tok_to_pair(slot, piece):
        return tok_copy(slot, c, piece, tp=partner)

    for first in range(2):
        for direction in range(2):
            tok_first(direction, (first + direction) % 2).start()

    def slab(buf, index):
        return buf.at[pl.ds(pl.multiple_of(index * 32, 32), 32)]

    def slab_copy(buf, recv, sent, index, target):
        ref = slab(buf, index)
        return pltpu.make_async_remote_copy(
            src_ref=ref,
            dst_ref=ref,
            send_sem=sent,
            recv_sem=recv,
            device_id={"sp": target},
            device_id_type=MESH,
        )

    def a_copy(gather, a, step):
        buf, recv_a, _, sent = gather
        target = sp_of(wrap(me_a + step), me_b)
        return slab_copy(buf, recv_a.at[a], sent, sp_of(a, me_b), target)

    def b_copy(gather, direction, j, b):
        buf, _, recv_b, sent = gather
        target = sp_of(me_a, wrap(me_b + 1 - 2 * direction))
        return slab_copy(buf, recv_b.at[b, j // 2], sent, sp_of(near(j), b), target)

    def wait_pair_of_slabs(gather, pair, b):
        buf, _, recv_b, sent = gather
        ref = buf.at[0:64]
        pltpu.make_async_remote_copy(
            src_ref=ref,
            dst_ref=ref,
            send_sem=sent,
            recv_sem=recv_b.at[b, pair],
            device_id={"tp": partner},
            device_id_type=MESH,
        ).wait_recv()

    def near(j):
        odd = j % 2
        dist = (j + 1) // 2
        return wrap(me_a + odd * dist - (1 - odd) * dist)

    def start_gather(gather, relay):
        b_copy(gather, 0, 0, me_b).start()
        b_copy(gather, 1, 0, me_b).start()

        def body(step, carry):
            a_copy(gather, me_a, step).start()
            return carry

        if relay:
            a_copy(gather, me_a, 1).start()
            a_copy(gather, me_a, -1).start()
        else:
            lax.fori_loop(1, RING, body, 0)

    def serve_a(gather, first, last, relay):
        def body(j, carry):
            a = near(j)
            a_copy(gather, a, 1).wait_recv()
            b_copy(gather, 0, j, me_b).start()
            b_copy(gather, 1, j, me_b).start()
            if relay:

                @pl.when(j % 2 == 0)
                def _():
                    a_copy(gather, a, 1).start()

                @pl.when((j % 2 == 1) & (j < 5))
                def _():
                    a_copy(gather, a, -1).start()

            return carry

        lax.fori_loop(first, last, body, 0)

    def serve_b(gather, step, first, last):
        def body(pair, carry):
            for direction in range(2):
                b = wrap(me_b - step if direction == 0 else me_b + step)
                wait_pair_of_slabs(gather, pair, b)

                def forward(b=b, direction=direction):
                    b_copy(gather, direction, 2 * pair, b).start()
                    b_copy(gather, direction, 2 * pair + 1, b).start()

                if step < 3:
                    forward()
                else:
                    pl.when(pair < 2 if direction == 0 else pair >= 2)(forward)
            return carry

        def body_last(pair, carry):
            wait_pair_of_slabs(gather, pair, wrap(me_b + step))
            return carry

        lax.fori_loop(first, last, body if step < 4 else body_last, 0)

    def end_gather(gather):
        buf, _, _, sent = gather
        ref = buf.at[0 : 63 * 32]
        pltpu.make_async_remote_copy(
            src_ref=ref,
            dst_ref=ref,
            send_sem=sent,
            recv_sem=stat_recv.at[0],
            device_id={"tp": partner},
            device_id_type=MESH,
        ).wait_send()

    gather_in = (win, in_recv_a, in_recv_b, in_sent)
    gather_out = (wout, out_recv_a, out_recv_b, out_sent)
    start_gather(gather_in, False)

    load_other.wait()
    norm_rows(pl.multiple_of(partner * HALF, HALF))
    for copy in load_out:
        copy.wait()
    for k in range(FS):
        at = pl.ds(pl.multiple_of(c * 512 + k * 128, 128), 128)
        wout[pl.ds(mine, 32), k * 256 : k * 256 + 128] = wao_ref[:, at]
        wout[pl.ds(mine, 32), k * 256 + 128 : (k + 1) * 256] = wco_ref[:, at]

    serve_a(gather_in, 1, 8, False)
    start_gather(gather_out, True)
    serve_b(gather_in, 1, 0, 4)

    lane = lax.broadcasted_iota(jnp.int32, (HALF, 128), 1)
    frequency = jnp.exp((lane % 16).astype(F32) * (-math.log(ROPE_BASE) / 16))
    for k in range(2):
        token = lax.broadcasted_iota(jnp.int32, (HALF, 128), 0) + k * HALF
        place = jnp.where(lane % 64 < 32, sp * 4 + token // 64, token % 64)
        angle = place.astype(F32) * frequency
        ctab[k * HALF : (k + 1) * HALF, :] = jnp.cos(angle)
        sine = jnp.sin(angle)
        stab[k * HALF : (k + 1) * HALF, :] = jnp.where(lane % 32 < 16, -sine, sine)

    @pl.when(sp == 0)
    def _():
        low[...] = jnp.zeros_like(low)

    @pl.when(sp == RING * RING - 1)
    def _():
        high[...] = jnp.zeros_like(high)

    serve_a(gather_out, 1, 3, True)
    serve_b(gather_in, 2, 0, 4)
    serve_a(gather_out, 3, 5, True)

    for direction in range(2):
        slot = fs_of(3 - 2 * direction)
        tok_to_pair(slot, direction).wait_recv()
        tok_second(direction).start()
        tok_to_pair(slot, direction).start()

    serve_b(gather_in, 3, 0, 4)
    serve_a(gather_out, 5, 7, True)

    for direction in range(2):
        slot = fs_of(3 - 2 * direction)
        tok_to_pair(slot, 1 - direction).wait_recv()
        tok_to_pair(slot, 1 - direction).start()

    serve_b(gather_in, 4, 0, 4)
    serve_a(gather_out, 7, 8, True)
    for copy in load_rest:
        copy.wait()

    def halo_copy(i, side):
        at = side * 144
        return pltpu.make_async_remote_copy(
            src_ref=kvg.at[i, at : at + 144],
            dst_ref=(low if side else high).at[i],
            send_sem=halo_sent[side],
            recv_sem=halo_recv.at[i, side],
            device_id={"sp": sp + 2 * side - 1},
            device_id_type=MESH,
        )

    lanes = lax.broadcasted_iota(jnp.int32, (TOK, 128), 1)

    def rotated(x, cosine, sine):
        other = jnp.where(lanes % 32 < 16, pltpu.roll(x, 112, 1), pltpu.roll(x, 16, 1))
        return x * cosine + other * sine

    def project(i):
        slot = fs_of(i)
        acc = jnp.dot(tok[slot], win[...], preferred_element_type=F32)
        cosine, sine = ctab[...], stab[...]
        query = rotated(acc[:, 0:128], cosine, sine).astype(BF16).astype(F32) * HEAD_DIM**-0.5
        qbuf[i, 0] = jnp.where(lanes < 64, query, 0.0).astype(BF16)
        qbuf[i, 1] = jnp.where(lanes < 64, pltpu.roll(query, 64, 1), 0.0).astype(BF16)
        pair = acc[:, 128:256]
        turned = rotated(pair, cosine, sine)
        kvg[i, 16:272] = jnp.where(lanes < 64, turned, pair).astype(BF16)
        glu = (acc[:, 256:384] * jax.nn.sigmoid(acc[:, 384:512])).astype(BF16)
        kvg[i, 0:16] = glu[0:16]
        kvg[i, 272:288] = glu[240:256]
        gext[i, 16:272] = glu.astype(F32)

        @pl.when(has_low)
        def _():
            halo_copy(i, 0).start()

        @pl.when(has_high)
        def _():
            halo_copy(i, 1).start()

    row_at = lax.broadcasted_iota(jnp.int32, (HALF, 256), 0)
    key_at = lax.broadcasted_iota(jnp.int32, (HALF, 256), 1)
    half_row = lax.broadcasted_iota(jnp.int32, (HALF, 128), 0)
    half_key = lax.broadcasted_iota(jnp.int32, (HALF, 128), 1)
    half_lane = half_key
    far = RING * TOK
    own_valid = (key_at - row_at <= WINDOW, key_at >= row_at)
    halo_valid = (
        half_key >= half_row + jnp.where(has_low, 0, far),
        half_key + jnp.where(has_high, 0, far) <= half_row,
    )

    head_lane = lax.broadcasted_iota(jnp.int32, (1, 8), 1)
    sinks = [
        jnp.sum(jnp.where(head_lane == 2 * f + h, sink_ref[...], 0.0), axis=-1, keepdims=True)
        for h in range(2)
    ]

    def mix(i):
        @pl.when(has_low)
        def _():
            halo_copy(i, 1).wait_recv()

        @pl.when(has_high)
        def _():
            halo_copy(i, 0).wait_recv()

        own_kv = kvg[i, 16:272]
        own_ones = jnp.where(
            lax.broadcasted_iota(jnp.int32, (TOK, 128), 1) < 64, jnp.ones_like(own_kv), own_kv
        )
        for block in range(2):
            near_kv = low[i, 0:128] if block == 0 else high[i, 16:144]
            near_ones = jnp.where(half_lane < 64, jnp.ones_like(near_kv), near_kv)
            heads = []
            for h in range(2):
                q = qbuf[i, h, block * HALF : (block + 1) * HALF]
                s_own = lax.dot_general(q, own_kv, NT, preferred_element_type=F32)
                s_near = lax.dot_general(q, near_kv, NT, preferred_element_type=F32)
                s_own = jnp.where(own_valid[block], s_own, NEGATIVE)
                s_near = jnp.where(halo_valid[block], s_near, NEGATIVE)
                sink = sinks[h]
                top = jnp.maximum(
                    jnp.maximum(s_own[:, 0:128], s_own[:, 128:256]), s_near
                )
                top = jnp.maximum(jnp.max(top, axis=-1, keepdims=True), sink)
                p_own = jnp.exp(s_own - top).astype(BF16)
                p_near = jnp.exp(s_near - top).astype(BF16)
                mixed = jnp.dot(p_own, own_ones, preferred_element_type=F32) + jnp.dot(
                    p_near, near_ones, preferred_element_type=F32
                )
                heads.append(mixed / (pltpu.roll(mixed, 64, 1) + jnp.exp(sink - top)))
            joined = jnp.where(half_lane < 64, pltpu.roll(heads[0], 64, 1), heads[1])
            sbuf[i, block * HALF : (block + 1) * HALF, 0:128] = joined.astype(BF16)

        gext[i, 0:16] = low[i, 128:144].astype(F32)
        gext[i, 272:288] = high[i, 0:16].astype(F32)

        for block in range(4):
            total = jnp.zeros((64, 128), F32)
            for k in range(TAPS):
                at = block * 64 + k + 1
                total = total + taps_ref[k : k + 1, cols] * gext[i, at : at + 64]
            sbuf[i, block * 64 : (block + 1) * 64, 128:256] = total.astype(BF16)

    def feat_copy(i):
        return pltpu.make_async_remote_copy(
            src_ref=sbuf.at[i],
            dst_ref=feat.at[f],
            send_sem=feat_sent,
            recv_sem=feat_recv.at[f],
            device_id={"fs": fs_of(i)},
            device_id_type=MESH,
        )

    def wait_pair(slot):
        tok_copy(slot, partner, 0, tp=partner).wait_recv()
        tok_copy(slot, partner, 1, tp=partner).wait_recv()

    project(0)
    serve_b(gather_out, 1, 0, 1)
    wait_pair(fs_of(1))
    project(1)
    serve_b(gather_out, 1, 1, 2)
    wait_pair(fs_of(3))
    project(3)
    for piece in range(2):
        tok_to_pair(fs_of(2), piece).wait_recv()
        tok_to_pair(fs_of(2), piece).start()
    serve_b(gather_out, 1, 2, 3)
    mix(0)
    feat[f] = sbuf[0]
    serve_b(gather_out, 1, 3, 4)
    wait_pair(fs_of(2))
    project(2)
    serve_b(gather_out, 2, 0, 1)
    mix(1)
    feat_copy(1).start()
    serve_b(gather_out, 2, 1, 3)
    mix(3)
    feat_copy(3).start()
    serve_b(gather_out, 2, 3, 4)
    serve_b(gather_out, 3, 0, 1)
    mix(2)
    feat_copy(2).start()
    serve_b(gather_out, 3, 1, 4)

    def feat_wait(src):
        pltpu.make_async_remote_copy(
            src_ref=sbuf.at[0],
            dst_ref=feat.at[src],
            send_sem=feat_sent,
            recv_sem=feat_recv.at[src],
            device_id={"tp": partner},
            device_id_type=MESH,
        ).wait_recv()

    for i in (1, 3, 2):
        feat_wait(fs_of(i))

    total = jnp.zeros((TOK, 1), F32)
    for k in range(FS):
        values = feat[k, :, 128:256].astype(F32) + bias_ref[:, k * 128 : (k + 1) * 128]
        cvals[:, k * 128 : (k + 1) * 128] = values
        total = total + jnp.sum(values, axis=-1, keepdims=True)
    here = total / 512.0
    around = jnp.zeros((TOK, 1), F32)
    for k in range(FS):
        centred = cvals[:, k * 128 : (k + 1) * 128] - here
        around = around + jnp.sum(centred * centred, axis=-1, keepdims=True)
    stat_out[...] = jnp.where(lanes < 64, here, around)
    stat_copy = pltpu.make_async_remote_copy(
        src_ref=stat_out,
        dst_ref=stat_in,
        send_sem=stat_sent,
        recv_sem=stat_recv.at[0],
        device_id={"tp": partner},
        device_id_type=MESH,
    )
    stat_copy.start()
    for k in range(FS):
        raw[:, k * 256 : k * 256 + 128] = feat[k, :, 0:128]
    stat_copy.wait_recv()
    there = stat_in[:, 0:1]
    gap = here - there
    centre = 0.5 * (here + there)
    spread = (around + stat_in[:, 64:65] + 256.0 * gap * gap) / 1024.0
    scale = lax.rsqrt(spread + EPSILON)
    for k in range(FS):
        at = slice(k * 128, (k + 1) * 128)
        v = (cvals[:, at] - centre) * scale * cgain_ref[:, at] + cshift_ref[:, at]
        raw[:, k * 256 + 128 : (k + 1) * 256] = (v / (1.0 + jnp.exp(-v))).astype(BF16)

    serve_b(gather_out, 4, 0, 4)

    def part_copy(n):
        return pltpu.make_async_remote_copy(
            src_ref=part_out.at[n],
            dst_ref=part_in.at[n],
            send_sem=part_sent,
            recv_sem=part_recv.at[n],
            device_id={"tp": partner},
            device_id_type=MESH,
        )

    for n in range(D // CHUNK):
        weights = wout[n * CHUNK : (n + 1) * CHUNK, :]
        part_out[n] = lax.dot_general(
            raw[other_half, :], weights, NT, preferred_element_type=F32
        ).astype(BF16)
        part_copy(n).start()
        part[n] = lax.dot_general(raw[own_half, :], weights, NT, preferred_element_type=F32)
    for n in range(D // CHUNK):
        part_copy(n).wait_recv()
        out_ref[:, n * CHUNK : (n + 1) * CHUNK] = (part[n] + part_in[n].astype(F32)).astype(BF16)

    def drain(ref, sent):
        pltpu.make_async_remote_copy(
            src_ref=ref,
            dst_ref=ref,
            send_sem=sent,
            recv_sem=stat_recv.at[0],
            device_id={"tp": partner},
            device_id_type=MESH,
        ).wait_send()

    drain(part_out, part_sent)
    stat_copy.wait_send()
    drain(sbuf.at[1:FS], feat_sent)

    @pl.when(has_low)
    def _():
        drain(kvg.at[:, 0:144], halo_sent[0])

    @pl.when(has_high)
    def _():
        drain(kvg.at[:, 144:288], halo_sent[1])

    drain(tok.at[0:3], tok_sent)
    end_gather(gather_in)
    end_gather(gather_out)


def local(
    tokens,
    norm_gain,
    w_query,
    w_key,
    w_value,
    w_conv_in,
    w_conv_gate,
    sink_logit,
    conv_taps,
    conv_bias,
    channel_gain,
    channel_shift,
    w_attn_out,
    w_conv_out,
):
    vmem = pl.BlockSpec(memory_space=pltpu.VMEM)
    anywhere = pl.BlockSpec(memory_space=pl.ANY)
    dma = pltpu.SemaphoreType.DMA
    args = (
        tokens,
        norm_gain.reshape(1, -1),
        w_query,
        w_key,
        w_value,
        w_conv_in,
        w_conv_gate,
        sink_logit.reshape(1, -1),
        conv_taps,
        conv_bias.reshape(1, -1),
        channel_gain.reshape(1, -1),
        channel_shift.reshape(1, -1),
        w_attn_out.T,
        w_conv_out.T,
    )
    return pl.pallas_call(
        kernel,
        out_shape=jax.ShapeDtypeStruct((HALF, D), BF16),
        in_specs=[anywhere] * len(args),
        out_specs=vmem,
        scratch_shapes=[pltpu.VMEM(a.shape, a.dtype) for a in args]
        + [
            pltpu.VMEM((FS, TOK, D), BF16),
            pltpu.VMEM((D, 512), BF16),
            pltpu.VMEM((D, 1024), BF16),
            pltpu.VMEM((TOK, 128), F32),
            pltpu.VMEM((TOK, 128), F32),
            pltpu.VMEM((FS, 2, TOK, 128), BF16),
            pltpu.VMEM((FS, 288, 128), BF16),
            pltpu.VMEM((FS, 288, 128), F32),
            pltpu.VMEM((FS, 144, 128), BF16),
            pltpu.VMEM((FS, 144, 128), BF16),
            pltpu.VMEM((FS, TOK, 256), BF16),
            pltpu.VMEM((FS, TOK, 256), BF16),
            pltpu.VMEM((TOK, 1024), BF16),
            pltpu.VMEM((TOK, 512), F32),
            pltpu.VMEM((TOK, 128), F32),
            pltpu.VMEM((TOK, 128), F32),
            pltpu.VMEM((D // CHUNK, HALF, CHUNK), F32),
            pltpu.VMEM((D // CHUNK, HALF, CHUNK), BF16),
            pltpu.VMEM((D // CHUNK, HALF, CHUNK), BF16),
            dma((15,)),
            dma((RING,)),
            dma((RING, 4)),
            dma((RING,)),
            dma((RING, 4)),
            dma((FS, 2, 2)),
            dma((FS, 2)),
            dma((FS,)),
            dma((1,)),
            dma((D // CHUNK,)),
            dma((8,)),
        ],
        compiler_params=pltpu.CompilerParams(
            collective_id=0, has_side_effects=True, vmem_limit_bytes=60 * 1024 * 1024
        ),
        name="fused",
    )(*args)


def solution(mesh):
    in_specs = (
        P(("fs", "sp"), None),
        P(),
        P("sp", "tp"),
        P("sp", "tp"),
        P("sp", "tp"),
        P("sp", "tp"),
        P("sp", "tp"),
        P("tp"),
        P(None, "tp"),
        P("tp"),
        P("tp"),
        P("tp"),
        P(None, "sp"),
        P(None, "sp"),
    )
    out_specs = P(("fs", "sp", "tp"), None)
    return jax.shard_map(local, mesh=mesh, in_specs=in_specs, out_specs=out_specs, check_vma=False)
```

```python
import functools
import math

import jax
import jax.numpy as jnp
from jax import lax
from jax.experimental import pallas as pl
from jax.experimental.pallas import tpu as pltpu
from jax.sharding import PartitionSpec as P

HEAD_DIM = 64
WINDOW = 128
EPSILON = 1e-06
NEGATIVE = -1e30
ROPE_BASE = 10000.0
TOK = 256
HALF = 128
D = 2048
TAPS = 31
RING = 8
FS = 4
CHUNK = 512
MESH = pl.DeviceIdType.MESH
NT = (((1,), (1,)), ((), ()))
F32 = jnp.float32
BF16 = jnp.bfloat16


def kernel(*refs):
    (
        tokens_hbm,
        gain_hbm,
        wq_hbm,
        wk_hbm,
        wv_hbm,
        wc_hbm,
        wg_hbm,
        sink_hbm,
        taps_hbm,
        bias_hbm,
        cgain_hbm,
        cshift_hbm,
        wao_hbm,
        wco_hbm,
        out_ref,
        tokens_ref,
        gain_ref,
        wq_ref,
        wk_ref,
        wv_ref,
        wc_ref,
        wg_ref,
        sink_ref,
        taps_ref,
        bias_ref,
        cgain_ref,
        cshift_ref,
        wao_ref,
        wco_ref,
        tok,
        win,
        wout,
        ctab,
        stab,
        qbuf,
        kvg,
        gext,
        low,
        high,
        sconv,
        satt,
        fconv,
        fatt,
        raw,
        cvals,
        stat_out,
        stat_in,
        part,
        part_out,
        part_in,
        load_sem,
        in_recv_a,
        in_recv_b,
        out_recv_a,
        out_recv_b,
        tok_recv,
        halo_recv,
        feat_recv,
        stat_recv,
        part_recv,
        send_sem,
    ) = refs
    in_sent, out_sent, tok_sent, conv_sent, att_sent, stat_sent, part_sent = (
        send_sem.at[k] for k in range(7)
    )
    halo_sent = (send_sem.at[7], send_sem.at[8])
    sp = lax.axis_index("sp")
    f = lax.axis_index("fs")
    c = lax.axis_index("tp")
    z, y = sp // RING, sp % RING
    me_a = (1 - c) * y + c * z
    me_b = (1 - c) * z + c * y
    partner = 1 - c

    def sp_of(a, b):
        return (1 - c) * (b * RING + a) + c * (a * RING + b)

    def wrap(v):
        return (v + 2 * RING) % RING

    def fs_of(step):
        return (f + step) % FS

    def load(k, src, dst):
        copy = pltpu.make_async_copy(src, dst, load_sem.at[k])
        copy.start()
        return copy

    own_half = pl.ds(pl.multiple_of(c * HALF, HALF), HALF)
    other_half = pl.ds(pl.multiple_of(partner * HALF, HALF), HALF)
    load_weights = [
        load(0, wq_hbm, wq_ref),
        load(1, wk_hbm, wk_ref),
        load(2, wv_hbm, wv_ref),
        load(3, wc_hbm, wc_ref),
        load(4, wg_hbm, wg_ref),
    ]
    load_own = [
        load(5, gain_hbm, gain_ref),
        load(6, tokens_hbm.at[own_half], tokens_ref.at[own_half]),
    ]
    load_other = load(7, tokens_hbm.at[other_half], tokens_ref.at[other_half])
    load_out = [load(8, wao_hbm, wao_ref), load(9, wco_hbm, wco_ref)]
    load_rest = [
        load(10, sink_hbm, sink_ref),
        load(11, taps_hbm, taps_ref),
        load(12, bias_hbm, bias_ref),
        load(13, cgain_hbm, cgain_ref),
        load(14, cshift_hbm, cshift_ref),
    ]

    has_low = sp > 0
    has_high = sp < RING * RING - 1

    barrier = pltpu.get_barrier_semaphore()

    def greet(**where):
        pl.semaphore_signal(barrier, inc=1, device_id=where, device_id_type=MESH)

    for step in range(1, RING):
        greet(sp=sp_of(wrap(me_a + step), me_b))
    greet(sp=sp_of(me_a, wrap(me_b + 1)))
    greet(sp=sp_of(me_a, wrap(me_b - 1)))
    for step in range(1, FS):
        greet(fs=fs_of(step))
    greet(tp=partner)

    greet(sp=(sp + 1) % (RING * RING))
    greet(sp=(sp + RING * RING - 1) % (RING * RING))

    lane32 = lax.broadcasted_iota(jnp.int32, (32, 128), 1)
    mine = pl.multiple_of(sp * 32, 32)
    cols = pl.ds(pl.multiple_of(f * 128, 128), 128)
    upper = f // 2
    for copy in load_weights:
        copy.wait()
    wk = wk_ref[...].astype(F32)
    wv = wv_ref[...].astype(F32)
    pick = (lane32 * 0 + upper) > 0
    wk = jnp.where(pick, pltpu.roll(wk, 64, 1), wk)
    wv = jnp.where(pick, wv, pltpu.roll(wv, 64, 1))
    win[pl.ds(mine, 32), 0:128] = wq_ref[:, cols]
    win[pl.ds(mine, 32), 128:256] = jnp.where(lane32 < 64, wk, wv).astype(BF16)
    win[pl.ds(mine, 32), 256:384] = wc_ref[:, cols]
    win[pl.ds(mine, 32), 384:512] = wg_ref[:, cols]

    def norm_rows(start):
        def body(i, carry):
            rows = pl.ds(pl.multiple_of(start + i * 16, 16), 16)
            x = tokens_ref[rows, :].astype(F32)
            scale = lax.rsqrt(jnp.mean(x * x, axis=-1, keepdims=True) + EPSILON)
            tok[f, rows, :] = (x * scale * gain_ref[...]).astype(BF16)
            return carry

        lax.fori_loop(0, HALF // 16, body, 0)

    for copy in load_own:
        copy.wait()
    norm_rows(pl.multiple_of(c * HALF, HALF))

    pl.semaphore_wait(barrier, RING - 1 + 2 + FS - 1 + 1 + 2)

    def tok_rows(half, piece):
        return pl.ds(pl.multiple_of(half * HALF + piece * 64, 64), 64)

    def tok_copy(slot, half, piece, **where):
        ref = tok.at[slot, tok_rows(half, piece)]
        return pltpu.make_async_remote_copy(
            src_ref=ref,
            dst_ref=ref,
            send_sem=tok_sent,
            recv_sem=tok_recv.at[slot, half, piece],
            device_id=where,
            device_id_type=MESH,
        )

    def tok_first(direction, piece):
        return tok_copy(f, c, piece, fs=fs_of(1 + 2 * direction))

    def tok_second(direction):
        slot = fs_of(3 - 2 * direction)
        return tok_copy(slot, c, direction, fs=fs_of(1 + 2 * direction))

    def tok_to_pair(slot, piece):
        return tok_copy(slot, c, piece, tp=partner)

    for first in range(2):
        for direction in range(2):
            tok_first(direction, (first + direction) % 2).start()

    def slab(buf, index):
        return buf.at[pl.ds(pl.multiple_of(index * 32, 32), 32)]

    def slab_copy(buf, recv, sent, index, target):
        ref = slab(buf, index)
        return pltpu.make_async_remote_copy(
            src_ref=ref,
            dst_ref=ref,
            send_sem=sent,
            recv_sem=recv,
            device_id={"sp": target},
            device_id_type=MESH,
        )

    def a_copy(gather, a, step):
        buf, recv_a, _, sent = gather
        target = sp_of(wrap(me_a + step), me_b)
        return slab_copy(buf, recv_a.at[a], sent, sp_of(a, me_b), target)

    def b_copy(gather, direction, j, b):
        buf, _, recv_b, sent = gather
        target = sp_of(me_a, wrap(me_b + 1 - 2 * direction))
        return slab_copy(buf, recv_b.at[b, j // 2], sent, sp_of(near(j), b), target)

    def wait_pair_of_slabs(gather, pair, b):
        buf, _, recv_b, sent = gather
        ref = buf.at[0:64]
        pltpu.make_async_remote_copy(
            src_ref=ref,
            dst_ref=ref,
            send_sem=sent,
            recv_sem=recv_b.at[b, pair],
            device_id={"tp": partner},
            device_id_type=MESH,
        ).wait_recv()

    def near(j):
        odd = j % 2
        dist = (j + 1) // 2
        return wrap(me_a + odd * dist - (1 - odd) * dist)

    def start_gather(gather, relay):
        b_copy(gather, 0, 0, me_b).start()
        b_copy(gather, 1, 0, me_b).start()

        def body(step, carry):
            a_copy(gather, me_a, step).start()
            return carry

        if relay:
            a_copy(gather, me_a, 1).start()
            a_copy(gather, me_a, -1).start()
        else:
            lax.fori_loop(1, RING, body, 0)

    def serve_a(gather, first, last, relay):
        def body(j, carry):
            a = near(j)
            a_copy(gather, a, 1).wait_recv()
            b_copy(gather, 0, j, me_b).start()
            b_copy(gather, 1, j, me_b).start()
            if relay:

                @pl.when(j % 2 == 0)
                def _():
                    a_copy(gather, a, 1).start()

                @pl.when((j % 2 == 1) & (j < 5))
                def _():
                    a_copy(gather, a, -1).start()

            return carry

        lax.fori_loop(first, last, body, 0)

    def serve_b(gather, step, first, last):
        def body(pair, carry):
            for direction in range(2):
                b = wrap(me_b - step if direction == 0 else me_b + step)
                wait_pair_of_slabs(gather, pair, b)

                def forward(b=b, direction=direction):
                    b_copy(gather, direction, 2 * pair, b).start()
                    b_copy(gather, direction, 2 * pair + 1, b).start()

                if step < 3:
                    forward()
                else:
                    pl.when(pair < 2 if direction == 0 else pair >= 2)(forward)
            return carry

        def body_last(pair, carry):
            wait_pair_of_slabs(gather, pair, wrap(me_b + step))
            return carry

        lax.fori_loop(first, last, body if step < 4 else body_last, 0)

    def end_gather(gather):
        buf, _, _, sent = gather
        ref = buf.at[0 : 63 * 32]
        pltpu.make_async_remote_copy(
            src_ref=ref,
            dst_ref=ref,
            send_sem=sent,
            recv_sem=stat_recv.at[0],
            device_id={"tp": partner},
            device_id_type=MESH,
        ).wait_send()

    gather_in = (win, in_recv_a, in_recv_b, in_sent)
    gather_out = (wout, out_recv_a, out_recv_b, out_sent)
    start_gather(gather_in, False)

    for copy in load_out:
        copy.wait()
    for k in range(FS):
        at = pl.ds(pl.multiple_of(c * 512 + k * 128, 128), 128)
        wout[pl.ds(mine, 32), k * 256 : k * 256 + 128] = wao_ref[:, at]
        wout[pl.ds(mine, 32), k * 256 + 128 : (k + 1) * 256] = wco_ref[:, at]

    start_gather(gather_out, True)
    load_other.wait()
    norm_rows(pl.multiple_of(partner * HALF, HALF))
    serve_a(gather_in, 1, 8, False)
    serve_a(gather_out, 1, 3, True)
    serve_b(gather_in, 1, 0, 4)

    lane = lax.broadcasted_iota(jnp.int32, (HALF, 128), 1)
    frequency = jnp.exp((lane % 16).astype(F32) * (-math.log(ROPE_BASE) / 16))
    for k in range(2):
        token = lax.broadcasted_iota(jnp.int32, (HALF, 128), 0) + k * HALF
        place = jnp.where(lane % 64 < 32, sp * 4 + token // 64, token % 64)
        angle = place.astype(F32) * frequency
        ctab[k * HALF : (k + 1) * HALF, :] = jnp.cos(angle)
        sine = jnp.sin(angle)
        stab[k * HALF : (k + 1) * HALF, :] = jnp.where(lane % 32 < 16, -sine, sine)

    @pl.when(sp == 0)
    def _():
        low[...] = jnp.zeros_like(low)

    @pl.when(sp == RING * RING - 1)
    def _():
        high[...] = jnp.zeros_like(high)

    serve_a(gather_out, 3, 5, True)
    serve_b(gather_in, 2, 0, 4)
    serve_a(gather_out, 5, 7, True)

    for direction in range(2):
        slot = fs_of(3 - 2 * direction)
        tok_to_pair(slot, direction).wait_recv()
        tok_second(direction).start()
        tok_to_pair(slot, direction).start()

    serve_b(gather_in, 3, 0, 4)
    serve_a(gather_out, 7, 8, True)

    for direction in range(2):
        slot = fs_of(3 - 2 * direction)
        tok_to_pair(slot, 1 - direction).wait_recv()
        tok_to_pair(slot, 1 - direction).start()

    serve_b(gather_out, 1, 0, 1)
    serve_b(gather_in, 4, 0, 4)
    for piece in range(2):
        tok_to_pair(fs_of(2), piece).wait_recv()
        tok_to_pair(fs_of(2), piece).start()
    for copy in load_rest:
        copy.wait()

    def halo_copy(i, side):
        at = side * 144
        return pltpu.make_async_remote_copy(
            src_ref=kvg.at[i, at : at + 144],
            dst_ref=(low if side else high).at[i],
            send_sem=halo_sent[side],
            recv_sem=halo_recv.at[i, side],
            device_id={"sp": sp + 2 * side - 1},
            device_id_type=MESH,
        )

    lanes = lax.broadcasted_iota(jnp.int32, (TOK, 128), 1)

    def rotated(x, cosine, sine):
        other = jnp.where(lanes % 32 < 16, pltpu.roll(x, 112, 1), pltpu.roll(x, 16, 1))
        return x * cosine + other * sine

    def project(i):
        slot = fs_of(i)
        acc = jnp.dot(tok[slot], win[...], preferred_element_type=F32)
        cosine, sine = ctab[...], stab[...]
        query = rotated(acc[:, 0:128], cosine, sine).astype(BF16).astype(F32) * HEAD_DIM**-0.5
        qbuf[i, 0] = jnp.where(lanes < 64, query, 0.0).astype(BF16)
        qbuf[i, 1] = jnp.where(lanes < 64, pltpu.roll(query, 64, 1), 0.0).astype(BF16)
        pair = acc[:, 128:256]
        turned = rotated(pair, cosine, sine)
        kvg[i, 16:272] = jnp.where(lanes < 64, turned, pair).astype(BF16)
        glu = (acc[:, 256:384] * jax.nn.sigmoid(acc[:, 384:512])).astype(BF16)
        kvg[i, 0:16] = glu[0:16]
        kvg[i, 272:288] = glu[240:256]
        gext[i, 16:272] = glu.astype(F32)

        @pl.when(has_low)
        def _():
            halo_copy(i, 0).start()

        @pl.when(has_high)
        def _():
            halo_copy(i, 1).start()

    row_at = lax.broadcasted_iota(jnp.int32, (HALF, 256), 0)
    key_at = lax.broadcasted_iota(jnp.int32, (HALF, 256), 1)
    half_row = lax.broadcasted_iota(jnp.int32, (HALF, 128), 0)
    half_key = lax.broadcasted_iota(jnp.int32, (HALF, 128), 1)
    half_lane = half_key
    far = RING * TOK
    own_valid = (key_at - row_at <= WINDOW, key_at >= row_at)
    halo_valid = (
        half_key >= half_row + jnp.where(has_low, 0, far),
        half_key + jnp.where(has_high, 0, far) <= half_row,
    )

    head_lane = lax.broadcasted_iota(jnp.int32, (1, 8), 1)
    sinks = [
        jnp.sum(jnp.where(head_lane == 2 * f + h, sink_ref[...], 0.0), axis=-1, keepdims=True)
        for h in range(2)
    ]

    def mix(i):
        own_kv = kvg[i, 16:272]
        own_ones = jnp.where(
            lax.broadcasted_iota(jnp.int32, (TOK, 128), 1) < 64, jnp.ones_like(own_kv), own_kv
        )
        for block in range(2):
            near_kv = low[i, 0:128] if block == 0 else high[i, 16:144]
            near_ones = jnp.where(half_lane < 64, jnp.ones_like(near_kv), near_kv)
            heads = []
            for h in range(2):
                q = qbuf[i, h, block * HALF : (block + 1) * HALF]
                s_own = lax.dot_general(q, own_kv, NT, preferred_element_type=F32)
                s_near = lax.dot_general(q, near_kv, NT, preferred_element_type=F32)
                s_own = jnp.where(own_valid[block], s_own, NEGATIVE)
                s_near = jnp.where(halo_valid[block], s_near, NEGATIVE)
                sink = sinks[h]
                top = jnp.maximum(
                    jnp.maximum(s_own[:, 0:128], s_own[:, 128:256]), s_near
                )
                top = jnp.maximum(jnp.max(top, axis=-1, keepdims=True), sink)
                p_own = jnp.exp(s_own - top).astype(BF16)
                p_near = jnp.exp(s_near - top).astype(BF16)
                mixed = jnp.dot(p_own, own_ones, preferred_element_type=F32) + jnp.dot(
                    p_near, near_ones, preferred_element_type=F32
                )
                heads.append(mixed / (pltpu.roll(mixed, 64, 1) + jnp.exp(sink - top)))
            joined = jnp.where(half_lane < 64, pltpu.roll(heads[0], 64, 1), heads[1])
            satt[i, block * HALF : (block + 1) * HALF] = joined.astype(BF16)

    def filter_taps(i):
        @pl.when(has_low)
        def _():
            halo_copy(i, 1).wait_recv()

        @pl.when(has_high)
        def _():
            halo_copy(i, 0).wait_recv()

        gext[i, 0:16] = low[i, 128:144].astype(F32)
        gext[i, 272:288] = high[i, 0:16].astype(F32)

        for block in range(4):
            total = jnp.zeros((64, 128), F32)
            for k in range(TAPS):
                at = block * 64 + k + 1
                total = total + taps_ref[k : k + 1, cols] * gext[i, at : at + 64]
            sconv[i, block * 64 : (block + 1) * 64] = total.astype(BF16)

    def feat_copy(kind, i):
        return pltpu.make_async_remote_copy(
            src_ref=(sconv, satt)[kind].at[i],
            dst_ref=(fconv, fatt)[kind].at[f],
            send_sem=(conv_sent, att_sent)[kind],
            recv_sem=feat_recv.at[kind, f],
            device_id={"fs": fs_of(i)},
            device_id_type=MESH,
        )

    def feat_wait(kind, src):
        pltpu.make_async_remote_copy(
            src_ref=(sconv, satt)[kind].at[0],
            dst_ref=(fconv, fatt)[kind].at[src],
            send_sem=(conv_sent, att_sent)[kind],
            recv_sem=feat_recv.at[kind, src],
            device_id={"tp": partner},
            device_id_type=MESH,
        ).wait_recv()

    def wait_pair(slot):
        tok_copy(slot, partner, 0, tp=partner).wait_recv()
        tok_copy(slot, partner, 1, tp=partner).wait_recv()

    serve_b(gather_out, 1, 1, 3)
    wait_pair(fs_of(1))
    project(1)
    wait_pair(fs_of(3))
    project(3)
    serve_b(gather_out, 1, 3, 4)
    wait_pair(fs_of(2))
    project(2)
    serve_b(gather_out, 2, 0, 1)
    project(0)
    serve_b(gather_out, 2, 1, 4)
    filter_taps(1)
    feat_copy(0, 1).start()
    filter_taps(3)
    feat_copy(0, 3).start()
    serve_b(gather_out, 3, 0, 1)
    filter_taps(2)
    feat_copy(0, 2).start()
    filter_taps(0)
    fconv[f] = sconv[0]
    serve_b(gather_out, 3, 1, 2)
    mix(2)
    feat_copy(1, 2).start()
    serve_b(gather_out, 3, 2, 3)
    mix(1)
    feat_copy(1, 1).start()
    serve_b(gather_out, 3, 3, 4)
    mix(3)
    feat_copy(1, 3).start()

    for i in range(1, FS):
        feat_wait(0, fs_of(i))

    total = jnp.zeros((TOK, 1), F32)
    for k in range(FS):
        values = jnp.concatenate(
            [fconv[k, other_half], fconv[k, own_half]], axis=0
        ).astype(F32)
        values = values + bias_ref[:, k * 128 : (k + 1) * 128]
        cvals[:, k * 128 : (k + 1) * 128] = values
        total = total + jnp.sum(values, axis=-1, keepdims=True)
    here = total / 512.0
    around = jnp.zeros((TOK, 1), F32)
    for k in range(FS):
        centred = cvals[:, k * 128 : (k + 1) * 128] - here
        around = around + jnp.sum(centred * centred, axis=-1, keepdims=True)
    stat_out[...] = jnp.where(lanes < 64, here, around)
    stat_copy = pltpu.make_async_remote_copy(
        src_ref=stat_out,
        dst_ref=stat_in,
        send_sem=stat_sent,
        recv_sem=stat_recv.at[0],
        device_id={"tp": partner},
        device_id_type=MESH,
    )
    stat_copy.start()
    mix(0)
    fatt[f] = satt[0]
    stat_copy.wait_recv()
    swapped = jnp.concatenate([stat_in[HALF:TOK, :], stat_in[0:HALF, :]], axis=0)
    there = swapped[:, 0:1]
    gap = here - there
    centre = 0.5 * (here + there)
    spread = (around + swapped[:, 64:65] + 256.0 * gap * gap) / 1024.0
    scale = lax.rsqrt(spread + EPSILON)
    for k in range(FS):
        at = slice(k * 128, (k + 1) * 128)
        v = (cvals[:, at] - centre) * scale * cgain_ref[:, at] + cshift_ref[:, at]
        raw[:, k * 256 + 128 : (k + 1) * 256] = (v / (1.0 + jnp.exp(-v))).astype(BF16)

    for i in range(1, FS):
        feat_wait(1, fs_of(i))
    for k in range(FS):
        raw[0:HALF, k * 256 : k * 256 + 128] = fatt[k, other_half]
        raw[HALF:TOK, k * 256 : k * 256 + 128] = fatt[k, own_half]

    serve_b(gather_out, 4, 0, 4)

    def part_copy(n):
        return pltpu.make_async_remote_copy(
            src_ref=part_out.at[n],
            dst_ref=part_in.at[n],
            send_sem=part_sent,
            recv_sem=part_recv.at[n],
            device_id={"tp": partner},
            device_id_type=MESH,
        )

    for n in range(D // CHUNK):
        weights = wout[n * CHUNK : (n + 1) * CHUNK, :]
        product = lax.dot_general(raw[...], weights, NT, preferred_element_type=F32)
        part_out[n] = product[0:HALF].astype(BF16)
        part_copy(n).start()
        part[n] = product[HALF:TOK]
    for n in range(D // CHUNK):
        part_copy(n).wait_recv()
        out_ref[:, n * CHUNK : (n + 1) * CHUNK] = (part[n] + part_in[n].astype(F32)).astype(BF16)

    def drain(ref, sent):
        pltpu.make_async_remote_copy(
            src_ref=ref,
            dst_ref=ref,
            send_sem=sent,
            recv_sem=stat_recv.at[0],
            device_id={"tp": partner},
            device_id_type=MESH,
        ).wait_send()

    drain(part_out, part_sent)
    stat_copy.wait_send()
    drain(sconv.at[1:FS], conv_sent)
    drain(satt.at[1:FS], att_sent)

    @pl.when(has_low)
    def _():
        drain(kvg.at[:, 0:144], halo_sent[0])

    @pl.when(has_high)
    def _():
        drain(kvg.at[:, 144:288], halo_sent[1])

    drain(tok.at[0:3], tok_sent)
    end_gather(gather_in)
    end_gather(gather_out)


def local(
    tokens,
    norm_gain,
    w_query,
    w_key,
    w_value,
    w_conv_in,
    w_conv_gate,
    sink_logit,
    conv_taps,
    conv_bias,
    channel_gain,
    channel_shift,
    w_attn_out,
    w_conv_out,
):
    vmem = pl.BlockSpec(memory_space=pltpu.VMEM)
    anywhere = pl.BlockSpec(memory_space=pl.ANY)
    dma = pltpu.SemaphoreType.DMA
    args = (
        tokens,
        norm_gain.reshape(1, -1),
        w_query,
        w_key,
        w_value,
        w_conv_in,
        w_conv_gate,
        sink_logit.reshape(1, -1),
        conv_taps,
        conv_bias.reshape(1, -1),
        channel_gain.reshape(1, -1),
        channel_shift.reshape(1, -1),
        w_attn_out.T,
        w_conv_out.T,
    )
    return pl.pallas_call(
        kernel,
        out_shape=jax.ShapeDtypeStruct((HALF, D), BF16),
        in_specs=[anywhere] * len(args),
        out_specs=vmem,
        scratch_shapes=[pltpu.VMEM(a.shape, a.dtype) for a in args]
        + [
            pltpu.VMEM((FS, TOK, D), BF16),
            pltpu.VMEM((D, 512), BF16),
            pltpu.VMEM((D, 1024), BF16),
            pltpu.VMEM((TOK, 128), F32),
            pltpu.VMEM((TOK, 128), F32),
            pltpu.VMEM((FS, 2, TOK, 128), BF16),
            pltpu.VMEM((FS, 288, 128), BF16),
            pltpu.VMEM((FS, 288, 128), F32),
            pltpu.VMEM((FS, 144, 128), BF16),
            pltpu.VMEM((FS, 144, 128), BF16),
            pltpu.VMEM((FS, TOK, 128), BF16),
            pltpu.VMEM((FS, TOK, 128), BF16),
            pltpu.VMEM((FS, TOK, 128), BF16),
            pltpu.VMEM((FS, TOK, 128), BF16),
            pltpu.VMEM((TOK, 1024), BF16),
            pltpu.VMEM((TOK, 512), F32),
            pltpu.VMEM((TOK, 128), F32),
            pltpu.VMEM((TOK, 128), F32),
            pltpu.VMEM((D // CHUNK, HALF, CHUNK), F32),
            pltpu.VMEM((D // CHUNK, HALF, CHUNK), BF16),
            pltpu.VMEM((D // CHUNK, HALF, CHUNK), BF16),
            dma((15,)),
            dma((RING,)),
            dma((RING, 4)),
            dma((RING,)),
            dma((RING, 4)),
            dma((FS, 2, 2)),
            dma((FS, 2)),
            dma((2, FS)),
            dma((1,)),
            dma((D // CHUNK,)),
            dma((9,)),
        ],
        compiler_params=pltpu.CompilerParams(
            collective_id=0, has_side_effects=True, vmem_limit_bytes=60 * 1024 * 1024
        ),
        name="fused",
    )(*args)


def solution(mesh):
    in_specs = (
        P(("fs", "sp"), None),
        P(),
        P("sp", "tp"),
        P("sp", "tp"),
        P("sp", "tp"),
        P("sp", "tp"),
        P("sp", "tp"),
        P("tp"),
        P(None, "tp"),
        P("tp"),
        P("tp"),
        P("tp"),
        P(None, "sp"),
        P(None, "sp"),
    )
    out_specs = P(("fs", "sp", "tp"), None)
    return jax.shard_map(local, mesh=mesh, in_specs=in_specs, out_specs=out_specs, check_vma=False)
```

```python
import functools
import math

import jax
import jax.numpy as jnp
from jax import lax
from jax.experimental import pallas as pl
from jax.experimental.pallas import tpu as pltpu
from jax.sharding import PartitionSpec as P

HEAD_DIM = 64
WINDOW = 128
EPSILON = 1e-06
NEGATIVE = -1e30
ROPE_BASE = 10000.0
TOK = 256
HALF = 128
D = 2048
TAPS = 31
RING = 8
FS = 4
CHUNK = 512
MESH = pl.DeviceIdType.MESH
NT = (((1,), (1,)), ((), ()))
F32 = jnp.float32
BF16 = jnp.bfloat16


def kernel(*refs):
    (
        tokens_hbm,
        gain_hbm,
        wq_hbm,
        wk_hbm,
        wv_hbm,
        wc_hbm,
        wg_hbm,
        sink_hbm,
        taps_hbm,
        bias_hbm,
        cgain_hbm,
        cshift_hbm,
        wao_hbm,
        wco_hbm,
        out_ref,
        tokens_ref,
        gain_ref,
        wq_ref,
        wk_ref,
        wv_ref,
        wc_ref,
        wg_ref,
        sink_ref,
        taps_ref,
        bias_ref,
        cgain_ref,
        cshift_ref,
        wao_ref,
        wco_ref,
        tok,
        win,
        wout,
        ctab,
        stab,
        qbuf,
        kvg,
        gext,
        low,
        high,
        sconv,
        satt,
        fconv,
        fatt,
        raw,
        cvals,
        stat_out,
        stat_in,
        part,
        part_out,
        part_in,
        load_sem,
        in_recv_a,
        in_recv_b,
        out_recv_a,
        out_recv_b,
        tok_recv,
        halo_recv,
        feat_recv,
        stat_recv,
        part_recv,
        send_sem,
    ) = refs
    in_sent, out_sent, tok_sent, conv_sent, att_sent, stat_sent, part_sent = (
        send_sem.at[k] for k in range(7)
    )
    halo_sent = (send_sem.at[7], send_sem.at[8])
    sp = lax.axis_index("sp")
    f = lax.axis_index("fs")
    c = lax.axis_index("tp")
    z, y = sp // RING, sp % RING
    me_a = (1 - c) * y + c * z
    me_b = (1 - c) * z + c * y
    partner = 1 - c

    def sp_of(a, b):
        return (1 - c) * (b * RING + a) + c * (a * RING + b)

    def wrap(v):
        return (v + 2 * RING) % RING

    def fs_of(step):
        return (f + step) % FS

    def load(k, src, dst):
        copy = pltpu.make_async_copy(src, dst, load_sem.at[k])
        copy.start()
        return copy

    own_half = pl.ds(pl.multiple_of(c * HALF, HALF), HALF)
    other_half = pl.ds(pl.multiple_of(partner * HALF, HALF), HALF)
    load_weights = [
        load(0, wq_hbm, wq_ref),
        load(1, wk_hbm, wk_ref),
        load(2, wv_hbm, wv_ref),
        load(3, wc_hbm, wc_ref),
        load(4, wg_hbm, wg_ref),
    ]
    load_own = [
        load(5, gain_hbm, gain_ref),
        load(6, tokens_hbm.at[own_half], tokens_ref.at[own_half]),
    ]
    load_other = load(7, tokens_hbm.at[other_half], tokens_ref.at[other_half])
    load_out = [load(8, wao_hbm, wao_ref), load(9, wco_hbm, wco_ref)]
    load_rest = [
        load(10, sink_hbm, sink_ref),
        load(11, taps_hbm, taps_ref),
        load(12, bias_hbm, bias_ref),
        load(13, cgain_hbm, cgain_ref),
        load(14, cshift_hbm, cshift_ref),
    ]

    has_low = sp > 0
    has_high = sp < RING * RING - 1

    barrier = pltpu.get_barrier_semaphore()

    def greet(**where):
        pl.semaphore_signal(barrier, inc=1, device_id=where, device_id_type=MESH)

    for step in range(1, RING):
        greet(sp=sp_of(wrap(me_a + step), me_b))
    greet(sp=sp_of(me_a, wrap(me_b + 1)))
    greet(sp=sp_of(me_a, wrap(me_b - 1)))
    for step in range(1, FS):
        greet(fs=fs_of(step))
    greet(tp=partner)

    greet(sp=(sp + 1) % (RING * RING))
    greet(sp=(sp + RING * RING - 1) % (RING * RING))

    lane32 = lax.broadcasted_iota(jnp.int32, (32, 128), 1)
    mine = pl.multiple_of(sp * 32, 32)
    cols = pl.ds(pl.multiple_of(f * 128, 128), 128)
    upper = f // 2
    for copy in load_weights:
        copy.wait()
    wk = wk_ref[...].astype(F32)
    wv = wv_ref[...].astype(F32)
    pick = (lane32 * 0 + upper) > 0
    wk = jnp.where(pick, pltpu.roll(wk, 64, 1), wk)
    wv = jnp.where(pick, wv, pltpu.roll(wv, 64, 1))
    win[pl.ds(mine, 32), 0:128] = wq_ref[:, cols]
    win[pl.ds(mine, 32), 128:256] = jnp.where(lane32 < 64, wk, wv).astype(BF16)
    win[pl.ds(mine, 32), 256:384] = wc_ref[:, cols]
    win[pl.ds(mine, 32), 384:512] = wg_ref[:, cols]

    def norm_rows(start):
        def body(i, carry):
            rows = pl.ds(pl.multiple_of(start + i * 16, 16), 16)
            x = tokens_ref[rows, :].astype(F32)
            scale = lax.rsqrt(jnp.mean(x * x, axis=-1, keepdims=True) + EPSILON)
            tok[f, rows, :] = (x * scale * gain_ref[...]).astype(BF16)
            return carry

        lax.fori_loop(0, HALF // 16, body, 0)

    pl.semaphore_wait(barrier, RING - 1 + 2 + FS - 1 + 1 + 2)

    def tok_rows(half, piece):
        return pl.ds(pl.multiple_of(half * HALF + piece * 64, 64), 64)

    def tok_copy(slot, half, piece, **where):
        ref = tok.at[slot, tok_rows(half, piece)]
        return pltpu.make_async_remote_copy(
            src_ref=ref,
            dst_ref=ref,
            send_sem=tok_sent,
            recv_sem=tok_recv.at[slot, half, piece],
            device_id=where,
            device_id_type=MESH,
        )

    def tok_first(direction, piece):
        return tok_copy(f, c, piece, fs=fs_of(1 + 2 * direction))

    def tok_second(direction):
        slot = fs_of(3 - 2 * direction)
        return tok_copy(slot, c, direction, fs=fs_of(1 + 2 * direction))

    def tok_to_pair(slot, piece):
        return tok_copy(slot, c, piece, tp=partner)

    def slab(buf, index):
        return buf.at[pl.ds(pl.multiple_of(index * 32, 32), 32)]

    def slab_copy(buf, recv, sent, index, target):
        ref = slab(buf, index)
        return pltpu.make_async_remote_copy(
            src_ref=ref,
            dst_ref=ref,
            send_sem=sent,
            recv_sem=recv,
            device_id={"sp": target},
            device_id_type=MESH,
        )

    def a_copy(gather, a, step):
        buf, recv_a, _, sent = gather
        target = sp_of(wrap(me_a + step), me_b)
        return slab_copy(buf, recv_a.at[a], sent, sp_of(a, me_b), target)

    def b_copy(gather, direction, j, b):
        buf, _, recv_b, sent = gather
        target = sp_of(me_a, wrap(me_b + 1 - 2 * direction))
        return slab_copy(buf, recv_b.at[b, j // 2], sent, sp_of(near(j), b), target)

    def wait_pair_of_slabs(gather, pair, b):
        buf, _, recv_b, sent = gather
        ref = buf.at[0:64]
        pltpu.make_async_remote_copy(
            src_ref=ref,
            dst_ref=ref,
            send_sem=sent,
            recv_sem=recv_b.at[b, pair],
            device_id={"tp": partner},
            device_id_type=MESH,
        ).wait_recv()

    def near(j):
        odd = j % 2
        dist = (j + 1) // 2
        return wrap(me_a + odd * dist - (1 - odd) * dist)

    def start_gather(gather, relay):
        b_copy(gather, 0, 0, me_b).start()
        b_copy(gather, 1, 0, me_b).start()

        def body(step, carry):
            a_copy(gather, me_a, 4 + (step // 2) * (2 * (step % 2) - 1)).start()
            return carry

        if relay:
            a_copy(gather, me_a, 1).start()
            a_copy(gather, me_a, -1).start()
        else:
            lax.fori_loop(1, RING, body, 0)

    def serve_a(gather, first, last, relay):
        def body(j, carry):
            a = near(j)
            a_copy(gather, a, 1).wait_recv()
            b_copy(gather, 0, j, me_b).start()
            b_copy(gather, 1, j, me_b).start()
            if relay:

                @pl.when(j % 2 == 0)
                def _():
                    a_copy(gather, a, 1).start()

                @pl.when((j % 2 == 1) & (j < 5))
                def _():
                    a_copy(gather, a, -1).start()

            return carry

        lax.fori_loop(first, last, body, 0)

    def serve_b(gather, step, first, last):
        def body(pair, carry):
            for direction in range(2):
                b = wrap(me_b - step if direction == 0 else me_b + step)
                wait_pair_of_slabs(gather, pair, b)

                def forward(b=b, direction=direction):
                    b_copy(gather, direction, 2 * pair, b).start()
                    b_copy(gather, direction, 2 * pair + 1, b).start()

                if step < 3:
                    forward()
                else:
                    pl.when(pair < 2 if direction == 0 else pair >= 2)(forward)
            return carry

        def body_last(pair, carry):
            wait_pair_of_slabs(gather, pair, wrap(me_b + step))
            return carry

        lax.fori_loop(first, last, body if step < 4 else body_last, 0)

    def end_gather(gather):
        buf, _, _, sent = gather
        ref = buf.at[0 : 63 * 32]
        pltpu.make_async_remote_copy(
            src_ref=ref,
            dst_ref=ref,
            send_sem=sent,
            recv_sem=stat_recv.at[0],
            device_id={"tp": partner},
            device_id_type=MESH,
        ).wait_send()

    gather_in = (win, in_recv_a, in_recv_b, in_sent)
    gather_out = (wout, out_recv_a, out_recv_b, out_sent)
    start_gather(gather_in, False)
    for copy in load_own:
        copy.wait()
    norm_rows(pl.multiple_of(c * HALF, HALF))
    for first in range(2):
        for direction in range(2):
            tok_first(direction, (first + direction) % 2).start()

    for copy in load_out:
        copy.wait()
    for k in range(FS):
        at = pl.ds(pl.multiple_of(c * 512 + k * 128, 128), 128)
        wout[pl.ds(mine, 32), k * 256 : k * 256 + 128] = wao_ref[:, at]
        wout[pl.ds(mine, 32), k * 256 + 128 : (k + 1) * 256] = wco_ref[:, at]

    start_gather(gather_out, True)
    load_other.wait()
    norm_rows(pl.multiple_of(partner * HALF, HALF))
    lane = lax.broadcasted_iota(jnp.int32, (HALF, 128), 1)
    frequency = jnp.exp((lane % 16).astype(F32) * (-math.log(ROPE_BASE) / 16))
    for k in range(2):
        token = lax.broadcasted_iota(jnp.int32, (HALF, 128), 0) + k * HALF
        place = jnp.where(lane % 64 < 32, sp * 4 + token // 64, token % 64)
        angle = place.astype(F32) * frequency
        ctab[k * HALF : (k + 1) * HALF, :] = jnp.cos(angle)
        sine = jnp.sin(angle)
        stab[k * HALF : (k + 1) * HALF, :] = jnp.where(lane % 32 < 16, -sine, sine)

    @pl.when(sp == 0)
    def _():
        low[...] = jnp.zeros_like(low)

    @pl.when(sp == RING * RING - 1)
    def _():
        high[...] = jnp.zeros_like(high)

    serve_a(gather_in, 1, 8, False)
    serve_a(gather_out, 1, 3, True)
    serve_b(gather_in, 1, 0, 4)

    serve_a(gather_out, 3, 5, True)
    serve_b(gather_in, 2, 0, 4)
    serve_a(gather_out, 5, 7, True)

    for direction in range(2):
        slot = fs_of(3 - 2 * direction)
        tok_to_pair(slot, direction).wait_recv()
        tok_second(direction).start()
        tok_to_pair(slot, direction).start()

    serve_b(gather_in, 3, 0, 4)
    serve_a(gather_out, 7, 8, True)

    for direction in range(2):
        slot = fs_of(3 - 2 * direction)
        tok_to_pair(slot, 1 - direction).wait_recv()
        tok_to_pair(slot, 1 - direction).start()

    serve_b(gather_out, 1, 0, 2)
    serve_b(gather_in, 4, 0, 4)
    for copy in load_rest:
        copy.wait()
    for piece in range(2):
        tok_to_pair(fs_of(2), piece).wait_recv()
        tok_to_pair(fs_of(2), piece).start()

    def halo_copy(i, side):
        at = side * 144
        return pltpu.make_async_remote_copy(
            src_ref=kvg.at[i, at : at + 144],
            dst_ref=(low if side else high).at[i],
            send_sem=halo_sent[side],
            recv_sem=halo_recv.at[i, side],
            device_id={"sp": sp + 2 * side - 1},
            device_id_type=MESH,
        )

    lanes = lax.broadcasted_iota(jnp.int32, (TOK, 128), 1)

    def rotated(x, cosine, sine):
        other = jnp.where(lanes % 32 < 16, pltpu.roll(x, 112, 1), pltpu.roll(x, 16, 1))
        return x * cosine + other * sine

    def project(i):
        slot = fs_of(i)
        acc = jnp.dot(tok[slot], win[...], preferred_element_type=F32)
        cosine, sine = ctab[...], stab[...]
        query = rotated(acc[:, 0:128], cosine, sine).astype(BF16).astype(F32) * HEAD_DIM**-0.5
        for h in range(2):
            head = query if h == 0 else pltpu.roll(query, 64, 1)
            head = jnp.where(lanes < 64, head, 0.0).astype(BF16)
            for block in range(2):
                qbuf[i, block, h * HALF : (h + 1) * HALF] = head[block * HALF : (block + 1) * HALF]
        pair = acc[:, 128:256]
        turned = rotated(pair, cosine, sine)
        kvg[i, 16:272] = jnp.where(lanes < 64, turned, pair).astype(BF16)
        glu = (acc[:, 256:384] * jax.nn.sigmoid(acc[:, 384:512])).astype(BF16)
        kvg[i, 0:16] = glu[0:16]
        kvg[i, 272:288] = glu[240:256]
        gext[i, 16:272] = glu.astype(F32)

        @pl.when(has_low)
        def _():
            halo_copy(i, 0).start()

        @pl.when(has_high)
        def _():
            halo_copy(i, 1).start()

    row_at = lax.broadcasted_iota(jnp.int32, (TOK, TOK), 0) % HALF
    key_at = lax.broadcasted_iota(jnp.int32, (TOK, TOK), 1)
    half_row = lax.broadcasted_iota(jnp.int32, (TOK, HALF), 0) % HALF
    half_key = lax.broadcasted_iota(jnp.int32, (TOK, HALF), 1)
    half_lane = lax.broadcasted_iota(jnp.int32, (HALF, 128), 1)
    far = RING * TOK
    own_valid = (key_at - row_at <= WINDOW, key_at >= row_at)
    halo_valid = (
        half_key >= half_row + jnp.where(has_low, 0, far),
        half_key + jnp.where(has_high, 0, far) <= half_row,
    )
    head_lane = lax.broadcasted_iota(jnp.int32, (1, 8), 1)
    sinks = [
        jnp.sum(jnp.where(head_lane == 2 * f + h, sink_ref[...], 0.0), axis=-1, keepdims=True)
        for h in range(2)
    ]
    first_head = lax.broadcasted_iota(jnp.int32, (TOK, 1), 0) < HALF
    sink = jnp.where(first_head, sinks[0], sinks[1])

    def mix(i):
        own_kv = kvg[i, 16:272]
        own_ones = jnp.where(lanes < 64, jnp.ones_like(own_kv), own_kv)
        for block in range(2):
            near_kv = low[i, 0:128] if block == 0 else high[i, 16:144]
            near_ones = jnp.where(half_lane < 64, jnp.ones_like(near_kv), near_kv)
            q = qbuf[i, block]
            s_own = lax.dot_general(q, own_kv, NT, preferred_element_type=F32)
            s_near = lax.dot_general(q, near_kv, NT, preferred_element_type=F32)
            s_own = jnp.where(own_valid[block], s_own, NEGATIVE)
            s_near = jnp.where(halo_valid[block], s_near, NEGATIVE)
            top = jnp.maximum(jnp.maximum(s_own[:, 0:128], s_own[:, 128:256]), s_near)
            top = jnp.maximum(jnp.max(top, axis=-1, keepdims=True), sink)
            p_own = jnp.exp(s_own - top).astype(BF16)
            p_near = jnp.exp(s_near - top).astype(BF16)
            mixed = jnp.dot(p_own, own_ones, preferred_element_type=F32) + jnp.dot(
                p_near, near_ones, preferred_element_type=F32
            )
            mixed = mixed / (pltpu.roll(mixed, 64, 1) + jnp.exp(sink - top))
            joined = jnp.where(half_lane < 64, pltpu.roll(mixed[0:HALF], 64, 1), mixed[HALF:TOK])
            satt[i, block * HALF : (block + 1) * HALF] = joined.astype(BF16)

    def filter_taps(i):
        @pl.when(has_low)
        def _():
            halo_copy(i, 1).wait_recv()

        @pl.when(has_high)
        def _():
            halo_copy(i, 0).wait_recv()

        gext[i, 0:16] = low[i, 128:144].astype(F32)
        gext[i, 272:288] = high[i, 0:16].astype(F32)

        for block in range(4):
            total = jnp.zeros((64, 128), F32)
            for k in range(TAPS):
                at = block * 64 + k + 1
                total = total + taps_ref[k : k + 1, cols] * gext[i, at : at + 64]
            sconv[i, block * 64 : (block + 1) * 64] = total.astype(BF16)

    def feat_copy(kind, i):
        return pltpu.make_async_remote_copy(
            src_ref=(sconv, satt)[kind].at[i],
            dst_ref=(fconv, fatt)[kind].at[f],
            send_sem=(conv_sent, att_sent)[kind],
            recv_sem=feat_recv.at[kind, f],
            device_id={"fs": fs_of(i)},
            device_id_type=MESH,
        )

    def feat_wait(kind, src):
        pltpu.make_async_remote_copy(
            src_ref=(sconv, satt)[kind].at[0],
            dst_ref=(fconv, fatt)[kind].at[src],
            send_sem=(conv_sent, att_sent)[kind],
            recv_sem=feat_recv.at[kind, src],
            device_id={"tp": partner},
            device_id_type=MESH,
        ).wait_recv()

    def wait_pair(slot):
        tok_copy(slot, partner, 0, tp=partner).wait_recv()
        tok_copy(slot, partner, 1, tp=partner).wait_recv()

    wait_pair(fs_of(1))
    project(1)
    serve_b(gather_out, 1, 2, 3)
    wait_pair(fs_of(3))
    project(3)
    serve_b(gather_out, 1, 3, 4)
    wait_pair(fs_of(2))
    project(2)
    serve_b(gather_out, 2, 0, 1)
    project(0)
    serve_b(gather_out, 2, 1, 2)
    filter_taps(1)
    feat_copy(0, 1).start()
    serve_b(gather_out, 2, 2, 3)
    filter_taps(3)
    feat_copy(0, 3).start()
    serve_b(gather_out, 2, 3, 4)
    filter_taps(2)
    feat_copy(0, 2).start()
    mix(1)
    feat_copy(1, 1).start()
    serve_b(gather_out, 3, 0, 1)
    mix(2)
    feat_copy(1, 2).start()
    serve_b(gather_out, 3, 1, 2)
    mix(3)
    feat_copy(1, 3).start()
    serve_b(gather_out, 3, 2, 3)
    filter_taps(0)
    fconv[f] = sconv[0]

    for i in range(1, FS):
        feat_wait(0, fs_of(i))

    total = jnp.zeros((TOK, 1), F32)
    for k in range(FS):
        values = jnp.concatenate(
            [fconv[k, other_half], fconv[k, own_half]], axis=0
        ).astype(F32)
        values = values + bias_ref[:, k * 128 : (k + 1) * 128]
        cvals[:, k * 128 : (k + 1) * 128] = values
        total = total + jnp.sum(values, axis=-1, keepdims=True)
    here = total / 512.0
    around = jnp.zeros((TOK, 1), F32)
    for k in range(FS):
        centred = cvals[:, k * 128 : (k + 1) * 128] - here
        around = around + jnp.sum(centred * centred, axis=-1, keepdims=True)
    stat_out[...] = jnp.where(lanes < 64, here, around)
    stat_copy = pltpu.make_async_remote_copy(
        src_ref=stat_out,
        dst_ref=stat_in,
        send_sem=stat_sent,
        recv_sem=stat_recv.at[0],
        device_id={"tp": partner},
        device_id_type=MESH,
    )
    stat_copy.start()
    serve_b(gather_out, 3, 3, 4)
    mix(0)
    fatt[f] = satt[0]
    stat_copy.wait_recv()
    swapped = jnp.concatenate([stat_in[HALF:TOK, :], stat_in[0:HALF, :]], axis=0)
    there = swapped[:, 0:1]
    gap = here - there
    centre = 0.5 * (here + there)
    spread = (around + swapped[:, 64:65] + 256.0 * gap * gap) / 1024.0
    scale = lax.rsqrt(spread + EPSILON)
    for k in range(FS):
        at = slice(k * 128, (k + 1) * 128)
        v = (cvals[:, at] - centre) * scale * cgain_ref[:, at] + cshift_ref[:, at]
        raw[:, k * 256 + 128 : (k + 1) * 256] = (v / (1.0 + jnp.exp(-v))).astype(BF16)

    for i in range(1, FS):
        feat_wait(1, fs_of(i))
    for k in range(FS):
        raw[0:HALF, k * 256 : k * 256 + 128] = fatt[k, other_half]
        raw[HALF:TOK, k * 256 : k * 256 + 128] = fatt[k, own_half]

    serve_b(gather_out, 4, 0, 4)

    def part_copy(n):
        return pltpu.make_async_remote_copy(
            src_ref=part_out.at[n],
            dst_ref=part_in.at[n],
            send_sem=part_sent,
            recv_sem=part_recv.at[n],
            device_id={"tp": partner},
            device_id_type=MESH,
        )

    for n in range(D // CHUNK):
        weights = wout[n * CHUNK : (n + 1) * CHUNK, :]
        product = lax.dot_general(raw[...], weights, NT, preferred_element_type=F32)
        part_out[n] = product[0:HALF].astype(BF16)
        part_copy(n).start()
        part[n] = product[HALF:TOK]
    for n in range(D // CHUNK):
        part_copy(n).wait_recv()
        out_ref[:, n * CHUNK : (n + 1) * CHUNK] = (part[n] + part_in[n].astype(F32)).astype(BF16)

    def drain(ref, sent):
        pltpu.make_async_remote_copy(
            src_ref=ref,
            dst_ref=ref,
            send_sem=sent,
            recv_sem=stat_recv.at[0],
            device_id={"tp": partner},
            device_id_type=MESH,
        ).wait_send()

    drain(part_out, part_sent)
    stat_copy.wait_send()
    drain(sconv.at[1:FS], conv_sent)
    drain(satt.at[1:FS], att_sent)

    @pl.when(has_low)
    def _():
        drain(kvg.at[:, 0:144], halo_sent[0])

    @pl.when(has_high)
    def _():
        drain(kvg.at[:, 144:288], halo_sent[1])

    drain(tok.at[0:3], tok_sent)
    end_gather(gather_in)
    end_gather(gather_out)


def local(
    tokens,
    norm_gain,
    w_query,
    w_key,
    w_value,
    w_conv_in,
    w_conv_gate,
    sink_logit,
    conv_taps,
    conv_bias,
    channel_gain,
    channel_shift,
    w_attn_out,
    w_conv_out,
):
    vmem = pl.BlockSpec(memory_space=pltpu.VMEM)
    anywhere = pl.BlockSpec(memory_space=pl.ANY)
    dma = pltpu.SemaphoreType.DMA
    args = (
        tokens,
        norm_gain.reshape(1, -1),
        w_query,
        w_key,
        w_value,
        w_conv_in,
        w_conv_gate,
        sink_logit.reshape(1, -1),
        conv_taps,
        conv_bias.reshape(1, -1),
        channel_gain.reshape(1, -1),
        channel_shift.reshape(1, -1),
        w_attn_out.T,
        w_conv_out.T,
    )
    return pl.pallas_call(
        kernel,
        out_shape=jax.ShapeDtypeStruct((HALF, D), BF16),
        in_specs=[anywhere] * len(args),
        out_specs=vmem,
        scratch_shapes=[pltpu.VMEM(a.shape, a.dtype) for a in args]
        + [
            pltpu.VMEM((FS, TOK, D), BF16),
            pltpu.VMEM((D, 512), BF16),
            pltpu.VMEM((D, 1024), BF16),
            pltpu.VMEM((TOK, 128), F32),
            pltpu.VMEM((TOK, 128), F32),
            pltpu.VMEM((FS, 2, TOK, 128), BF16),
            pltpu.VMEM((FS, 288, 128), BF16),
            pltpu.VMEM((FS, 288, 128), F32),
            pltpu.VMEM((FS, 144, 128), BF16),
            pltpu.VMEM((FS, 144, 128), BF16),
            pltpu.VMEM((FS, TOK, 128), BF16),
            pltpu.VMEM((FS, TOK, 128), BF16),
            pltpu.VMEM((FS, TOK, 128), BF16),
            pltpu.VMEM((FS, TOK, 128), BF16),
            pltpu.VMEM((TOK, 1024), BF16),
            pltpu.VMEM((TOK, 512), F32),
            pltpu.VMEM((TOK, 128), F32),
            pltpu.VMEM((TOK, 128), F32),
            pltpu.VMEM((D // CHUNK, HALF, CHUNK), F32),
            pltpu.VMEM((D // CHUNK, HALF, CHUNK), BF16),
            pltpu.VMEM((D // CHUNK, HALF, CHUNK), BF16),
            dma((15,)),
            dma((RING,)),
            dma((RING, 4)),
            dma((RING,)),
            dma((RING, 4)),
            dma((FS, 2, 2)),
            dma((FS, 2)),
            dma((2, FS)),
            dma((1,)),
            dma((D // CHUNK,)),
            dma((9,)),
        ],
        compiler_params=pltpu.CompilerParams(
            collective_id=0, has_side_effects=True, vmem_limit_bytes=32 * 1024 * 1024
        ),
        name="fused",
    )(*(pltpu.with_memory_space_constraint(a, pltpu.HBM) for a in args))


def solution(mesh):
    in_specs = (
        P(("fs", "sp"), None),
        P(),
        P("sp", "tp"),
        P("sp", "tp"),
        P("sp", "tp"),
        P("sp", "tp"),
        P("sp", "tp"),
        P("tp"),
        P(None, "tp"),
        P("tp"),
        P("tp"),
        P("tp"),
        P(None, "sp"),
        P(None, "sp"),
    )
    out_specs = P(("fs", "sp", "tp"), None)
    return jax.shard_map(local, mesh=mesh, in_specs=in_specs, out_specs=out_specs, check_vma=False)
```

```python
import functools
import math

import jax
import jax.numpy as jnp
from jax import lax
from jax.experimental import pallas as pl
from jax.experimental.pallas import tpu as pltpu
from jax.sharding import PartitionSpec as P

HEAD_DIM = 64
WINDOW = 128
EPSILON = 1e-06
NEGATIVE = -1e30
ROPE_BASE = 10000.0
TOK = 256
HALF = 128
D = 2048
TAPS = 31
RING = 8
FS = 4
CHUNK = 512
MESH = pl.DeviceIdType.MESH
NT = (((1,), (1,)), ((), ()))
F32 = jnp.float32
BF16 = jnp.bfloat16


def kernel(*refs):
    (
        tokens_hbm,
        gain_hbm,
        wq_hbm,
        wk_hbm,
        wv_hbm,
        wc_hbm,
        wg_hbm,
        sink_hbm,
        taps_hbm,
        bias_hbm,
        cgain_hbm,
        cshift_hbm,
        wao_hbm,
        wco_hbm,
        out_ref,
        tokens_ref,
        gain_ref,
        wq_ref,
        wk_ref,
        wv_ref,
        wc_ref,
        wg_ref,
        sink_ref,
        taps_ref,
        bias_ref,
        cgain_ref,
        cshift_ref,
        wao_ref,
        wco_ref,
        tok,
        win,
        wout,
        ctab,
        stab,
        qbuf,
        kvg,
        gext,
        low,
        high,
        sconv,
        satt,
        fconv,
        fatt,
        raw,
        cvals,
        stat_out,
        stat_in,
        part,
        part_out,
        part_in,
        load_sem,
        in_recv_a,
        in_recv_b,
        out_recv_a,
        out_recv_b,
        tok_recv,
        halo_recv,
        feat_recv,
        stat_recv,
        part_recv,
        send_sem,
    ) = refs
    in_sent, out_sent, tok_sent, conv_sent, att_sent, stat_sent, part_sent = (
        send_sem.at[k] for k in range(7)
    )
    halo_sent = (send_sem.at[7], send_sem.at[8])
    sp = lax.axis_index("sp")
    f = lax.axis_index("fs")
    c = lax.axis_index("tp")
    z, y = sp // RING, sp % RING
    me_a = (1 - c) * y + c * z
    me_b = (1 - c) * z + c * y
    partner = 1 - c

    def sp_of(a, b):
        return (1 - c) * (b * RING + a) + c * (a * RING + b)

    def wrap(v):
        return (v + 2 * RING) % RING

    def fs_of(step):
        return (f + step) % FS

    def load(k, src, dst):
        copy = pltpu.make_async_copy(src, dst, load_sem.at[k])
        copy.start()
        return copy

    own_half = pl.ds(pl.multiple_of(c * HALF, HALF), HALF)
    other_half = pl.ds(pl.multiple_of(partner * HALF, HALF), HALF)
    load_weights = [
        load(0, wq_hbm, wq_ref),
        load(1, wk_hbm, wk_ref),
        load(2, wv_hbm, wv_ref),
        load(3, wc_hbm, wc_ref),
        load(4, wg_hbm, wg_ref),
    ]
    load_own = [
        load(5, gain_hbm, gain_ref),
        load(6, tokens_hbm.at[own_half], tokens_ref.at[own_half]),
    ]
    load_other = load(7, tokens_hbm.at[other_half], tokens_ref.at[other_half])
    load_out = [load(8, wao_hbm, wao_ref), load(9, wco_hbm, wco_ref)]
    load_rest = [
        load(10, sink_hbm, sink_ref),
        load(11, taps_hbm, taps_ref),
        load(12, bias_hbm, bias_ref),
        load(13, cgain_hbm, cgain_ref),
        load(14, cshift_hbm, cshift_ref),
    ]

    has_low = sp > 0
    has_high = sp < RING * RING - 1

    barrier = pltpu.get_barrier_semaphore()

    def greet(**where):
        pl.semaphore_signal(barrier, inc=1, device_id=where, device_id_type=MESH)

    for step in range(1, RING):
        greet(sp=sp_of(wrap(me_a + step), me_b))
    greet(sp=sp_of(me_a, wrap(me_b + 1)))
    greet(sp=sp_of(me_a, wrap(me_b - 1)))
    for step in range(1, FS):
        greet(fs=fs_of(step))
    greet(tp=partner)

    greet(sp=(sp + 1) % (RING * RING))
    greet(sp=(sp + RING * RING - 1) % (RING * RING))

    lane32 = lax.broadcasted_iota(jnp.int32, (32, 128), 1)
    mine = pl.multiple_of(sp * 32, 32)
    cols = pl.ds(pl.multiple_of(f * 128, 128), 128)
    upper = f // 2
    for copy in load_weights:
        copy.wait()
    wk = wk_ref[...].astype(F32)
    wv = wv_ref[...].astype(F32)
    pick = (lane32 * 0 + upper) > 0
    wk = jnp.where(pick, pltpu.roll(wk, 64, 1), wk)
    wv = jnp.where(pick, wv, pltpu.roll(wv, 64, 1))
    win[pl.ds(mine, 32), 0:128] = wq_ref[:, cols]
    win[pl.ds(mine, 32), 128:256] = jnp.where(lane32 < 64, wk, wv).astype(BF16)
    win[pl.ds(mine, 32), 256:384] = wc_ref[:, cols]
    win[pl.ds(mine, 32), 384:512] = wg_ref[:, cols]

    def norm_rows(start):
        def body(i, carry):
            rows = pl.ds(pl.multiple_of(start + i * 16, 16), 16)
            x = tokens_ref[rows, :].astype(F32)
            scale = lax.rsqrt(jnp.mean(x * x, axis=-1, keepdims=True) + EPSILON)
            tok[f, rows, :] = (x * scale * gain_ref[...]).astype(BF16)
            return carry

        lax.fori_loop(0, HALF // 16, body, 0)

    pl.semaphore_wait(barrier, RING - 1 + 2 + FS - 1 + 1 + 2)

    def tok_rows(half, piece):
        return pl.ds(pl.multiple_of(half * HALF + piece * 64, 64), 64)

    def tok_copy(slot, half, piece, **where):
        ref = tok.at[slot, tok_rows(half, piece)]
        return pltpu.make_async_remote_copy(
            src_ref=ref,
            dst_ref=ref,
            send_sem=tok_sent,
            recv_sem=tok_recv.at[slot, half, piece],
            device_id=where,
            device_id_type=MESH,
        )

    def tok_first(direction, piece):
        return tok_copy(f, c, piece, fs=fs_of(1 + 2 * direction))

    def tok_second(direction):
        slot = fs_of(3 - 2 * direction)
        return tok_copy(slot, c, direction, fs=fs_of(1 + 2 * direction))

    def tok_to_pair(slot, piece):
        return tok_copy(slot, c, piece, tp=partner)

    def slab(buf, index):
        return buf.at[pl.ds(pl.multiple_of(index * 32, 32), 32)]

    def slab_copy(buf, recv, sent, index, target):
        ref = slab(buf, index)
        return pltpu.make_async_remote_copy(
            src_ref=ref,
            dst_ref=ref,
            send_sem=sent,
            recv_sem=recv,
            device_id={"sp": target},
            device_id_type=MESH,
        )

    def a_copy(gather, a, step):
        buf, recv_a, _, sent = gather
        target = sp_of(wrap(me_a + step), me_b)
        return slab_copy(buf, recv_a.at[a], sent, sp_of(a, me_b), target)

    def b_copy(gather, direction, j, b):
        buf, _, recv_b, sent = gather
        target = sp_of(me_a, wrap(me_b + 1 - 2 * direction))
        return slab_copy(buf, recv_b.at[b, j // 2], sent, sp_of(near(j), b), target)

    def wait_pair_of_slabs(gather, pair, b):
        buf, _, recv_b, sent = gather
        ref = buf.at[0:64]
        pltpu.make_async_remote_copy(
            src_ref=ref,
            dst_ref=ref,
            send_sem=sent,
            recv_sem=recv_b.at[b, pair],
            device_id={"tp": partner},
            device_id_type=MESH,
        ).wait_recv()

    def near(j):
        odd = j % 2
        dist = (j + 1) // 2
        return wrap(me_a + odd * dist - (1 - odd) * dist)

    def start_gather(gather, relay):
        b_copy(gather, 0, 0, me_b).start()
        b_copy(gather, 1, 0, me_b).start()

        if relay:
            a_copy(gather, me_a, 1).start()
            a_copy(gather, me_a, -1).start()
        else:
            for step in (1, -1, 4, 3, -3, 2, -2):
                a_copy(gather, me_a, step).start()

    def serve_a(gather, first, last, relay):
        def body(j, carry):
            a = near(j)
            a_copy(gather, a, 1).wait_recv()
            b_copy(gather, 0, j, me_b).start()
            b_copy(gather, 1, j, me_b).start()
            if relay:

                @pl.when(j % 2 == 0)
                def _():
                    a_copy(gather, a, 1).start()

                @pl.when((j % 2 == 1) & (j < 5))
                def _():
                    a_copy(gather, a, -1).start()

            return carry

        lax.fori_loop(first, last, body, 0)

    def serve_b(gather, step, first, last):
        def body(pair, carry):
            for direction in range(2):
                b = wrap(me_b - step if direction == 0 else me_b + step)
                wait_pair_of_slabs(gather, pair, b)

                def forward(b=b, direction=direction):
                    b_copy(gather, direction, 2 * pair, b).start()
                    b_copy(gather, direction, 2 * pair + 1, b).start()

                if step < 3:
                    forward()
                else:
                    pl.when(pair < 2 if direction == 0 else pair >= 2)(forward)
            return carry

        def body_last(pair, carry):
            wait_pair_of_slabs(gather, pair, wrap(me_b + step))
            return carry

        lax.fori_loop(first, last, body if step < 4 else body_last, 0)

    def end_gather(gather):
        buf, _, _, sent = gather
        ref = buf.at[0 : 63 * 32]
        pltpu.make_async_remote_copy(
            src_ref=ref,
            dst_ref=ref,
            send_sem=sent,
            recv_sem=stat_recv.at[0],
            device_id={"tp": partner},
            device_id_type=MESH,
        ).wait_send()

    gather_in = (win, in_recv_a, in_recv_b, in_sent)
    gather_out = (wout, out_recv_a, out_recv_b, out_sent)
    start_gather(gather_in, False)
    for copy in load_own:
        copy.wait()
    norm_rows(pl.multiple_of(c * HALF, HALF))
    for first in range(2):
        for direction in range(2):
            tok_first(direction, (first + direction) % 2).start()

    for copy in load_out:
        copy.wait()
    for k in range(FS):
        at = pl.ds(pl.multiple_of(c * 512 + k * 128, 128), 128)
        wout[pl.ds(mine, 32), k * 256 : k * 256 + 128] = wao_ref[:, at]
        wout[pl.ds(mine, 32), k * 256 + 128 : (k + 1) * 256] = wco_ref[:, at]

    start_gather(gather_out, True)
    load_other.wait()
    norm_rows(pl.multiple_of(partner * HALF, HALF))
    lane = lax.broadcasted_iota(jnp.int32, (HALF, 128), 1)
    frequency = jnp.exp((lane % 16).astype(F32) * (-math.log(ROPE_BASE) / 16))
    for k in range(2):
        token = lax.broadcasted_iota(jnp.int32, (HALF, 128), 0) + k * HALF
        place = jnp.where(lane % 64 < 32, sp * 4 + token // 64, token % 64)
        angle = place.astype(F32) * frequency
        ctab[k * HALF : (k + 1) * HALF, :] = jnp.cos(angle)
        sine = jnp.sin(angle)
        stab[k * HALF : (k + 1) * HALF, :] = jnp.where(lane % 32 < 16, -sine, sine)

    @pl.when(sp == 0)
    def _():
        low[...] = jnp.zeros_like(low)

    @pl.when(sp == RING * RING - 1)
    def _():
        high[...] = jnp.zeros_like(high)

    serve_a(gather_in, 1, 8, False)
    serve_a(gather_out, 1, 3, True)
    serve_b(gather_in, 1, 0, 4)

    serve_a(gather_out, 3, 5, True)
    serve_b(gather_in, 2, 0, 4)
    serve_a(gather_out, 5, 7, True)

    for direction in range(2):
        slot = fs_of(3 - 2 * direction)
        tok_to_pair(slot, direction).wait_recv()
        tok_second(direction).start()
        tok_to_pair(slot, direction).start()

    serve_b(gather_in, 3, 0, 4)
    serve_a(gather_out, 7, 8, True)

    for direction in range(2):
        slot = fs_of(3 - 2 * direction)
        tok_to_pair(slot, 1 - direction).wait_recv()
        tok_to_pair(slot, 1 - direction).start()

    serve_b(gather_out, 1, 0, 3)
    for piece in range(2):
        tok_to_pair(fs_of(2), piece).wait_recv()
        tok_to_pair(fs_of(2), piece).start()
    serve_b(gather_in, 4, 0, 4)
    for copy in load_rest:
        copy.wait()

    def halo_copy(i, side):
        at = side * 144
        return pltpu.make_async_remote_copy(
            src_ref=kvg.at[i, at : at + 144],
            dst_ref=(low if side else high).at[i],
            send_sem=halo_sent[side],
            recv_sem=halo_recv.at[i, side],
            device_id={"sp": sp + 2 * side - 1},
            device_id_type=MESH,
        )

    lanes = lax.broadcasted_iota(jnp.int32, (TOK, 128), 1)

    def rotated(x, cosine, sine):
        other = jnp.where(lanes % 32 < 16, pltpu.roll(x, 112, 1), pltpu.roll(x, 16, 1))
        return x * cosine + other * sine

    def project(i):
        slot = fs_of(i)
        acc = jnp.dot(tok[slot], win[...], preferred_element_type=F32)
        cosine, sine = ctab[...], stab[...]
        query = rotated(acc[:, 0:128], cosine, sine).astype(BF16).astype(F32) * HEAD_DIM**-0.5
        for h in range(2):
            head = query if h == 0 else pltpu.roll(query, 64, 1)
            head = jnp.where(lanes < 64, head, 0.0).astype(BF16)
            for block in range(2):
                qbuf[i, block, h * HALF : (h + 1) * HALF] = head[block * HALF : (block + 1) * HALF]
        pair = acc[:, 128:256]
        turned = rotated(pair, cosine, sine)
        kvg[i, 16:272] = jnp.where(lanes < 64, turned, pair).astype(BF16)
        glu = (acc[:, 256:384] * jax.nn.sigmoid(acc[:, 384:512])).astype(BF16)
        kvg[i, 0:16] = glu[0:16]
        kvg[i, 272:288] = glu[240:256]
        gext[i, 16:272] = glu.astype(F32)

        @pl.when(has_low)
        def _():
            halo_copy(i, 0).start()

        @pl.when(has_high)
        def _():
            halo_copy(i, 1).start()

    row_at = lax.broadcasted_iota(jnp.int32, (TOK, TOK), 0) % HALF
    key_at = lax.broadcasted_iota(jnp.int32, (TOK, TOK), 1)
    half_row = lax.broadcasted_iota(jnp.int32, (TOK, HALF), 0) % HALF
    half_key = lax.broadcasted_iota(jnp.int32, (TOK, HALF), 1)
    half_lane = lax.broadcasted_iota(jnp.int32, (HALF, 128), 1)
    far = RING * TOK
    own_valid = (key_at - row_at <= WINDOW, key_at >= row_at)
    halo_valid = (
        half_key >= half_row + jnp.where(has_low, 0, far),
        half_key + jnp.where(has_high, 0, far) <= half_row,
    )
    head_lane = lax.broadcasted_iota(jnp.int32, (1, 8), 1)
    sinks = [
        jnp.sum(jnp.where(head_lane == 2 * f + h, sink_ref[...], 0.0), axis=-1, keepdims=True)
        for h in range(2)
    ]
    first_head = lax.broadcasted_iota(jnp.int32, (TOK, 1), 0) < HALF
    sink = jnp.where(first_head, sinks[0], sinks[1])

    def mix(i):
        own_kv = kvg[i, 16:272]
        own_ones = jnp.where(lanes < 64, jnp.ones_like(own_kv), own_kv)
        for block in range(2):
            near_kv = low[i, 0:128] if block == 0 else high[i, 16:144]
            near_ones = jnp.where(half_lane < 64, jnp.ones_like(near_kv), near_kv)
            q = qbuf[i, block]
            s_own = lax.dot_general(q, own_kv, NT, preferred_element_type=F32)
            s_near = lax.dot_general(q, near_kv, NT, preferred_element_type=F32)
            s_own = jnp.where(own_valid[block], s_own, NEGATIVE)
            s_near = jnp.where(halo_valid[block], s_near, NEGATIVE)
            top = jnp.maximum(jnp.maximum(s_own[:, 0:128], s_own[:, 128:256]), s_near)
            top = jnp.maximum(jnp.max(top, axis=-1, keepdims=True), sink)
            p_own = jnp.exp(s_own - top).astype(BF16)
            p_near = jnp.exp(s_near - top).astype(BF16)
            mixed = jnp.dot(p_own, own_ones, preferred_element_type=F32) + jnp.dot(
                p_near, near_ones, preferred_element_type=F32
            )
            mixed = mixed / (pltpu.roll(mixed, 64, 1) + jnp.exp(sink - top))
            joined = jnp.where(half_lane < 64, pltpu.roll(mixed[0:HALF], 64, 1), mixed[HALF:TOK])
            satt[i, block * HALF : (block + 1) * HALF] = joined.astype(BF16)

    def filter_taps(i):
        @pl.when(has_low)
        def _():
            halo_copy(i, 1).wait_recv()

        @pl.when(has_high)
        def _():
            halo_copy(i, 0).wait_recv()

        gext[i, 0:16] = low[i, 128:144].astype(F32)
        gext[i, 272:288] = high[i, 0:16].astype(F32)

        for block in range(4):
            total = jnp.zeros((64, 128), F32)
            for k in range(TAPS):
                at = block * 64 + k + 1
                total = total + taps_ref[k : k + 1, cols] * gext[i, at : at + 64]
            sconv[i, block * 64 : (block + 1) * 64] = total.astype(BF16)

    def feat_copy(kind, i):
        return pltpu.make_async_remote_copy(
            src_ref=(sconv, satt)[kind].at[i],
            dst_ref=(fconv, fatt)[kind].at[f],
            send_sem=(conv_sent, att_sent)[kind],
            recv_sem=feat_recv.at[kind, f],
            device_id={"fs": fs_of(i)},
            device_id_type=MESH,
        )

    def feat_wait(kind, src):
        pltpu.make_async_remote_copy(
            src_ref=(sconv, satt)[kind].at[0],
            dst_ref=(fconv, fatt)[kind].at[src],
            send_sem=(conv_sent, att_sent)[kind],
            recv_sem=feat_recv.at[kind, src],
            device_id={"tp": partner},
            device_id_type=MESH,
        ).wait_recv()

    def wait_pair(slot):
        tok_copy(slot, partner, 0, tp=partner).wait_recv()
        tok_copy(slot, partner, 1, tp=partner).wait_recv()

    wait_pair(fs_of(1))
    project(1)
    serve_b(gather_out, 1, 3, 4)
    wait_pair(fs_of(3))
    project(3)
    wait_pair(fs_of(2))
    project(2)
    serve_b(gather_out, 2, 0, 1)
    project(0)
    serve_b(gather_out, 2, 1, 4)
    filter_taps(1)
    feat_copy(0, 1).start()
    filter_taps(3)
    feat_copy(0, 3).start()
    mix(1)
    feat_copy(1, 1).start()
    serve_b(gather_out, 3, 0, 1)
    filter_taps(2)
    feat_copy(0, 2).start()
    mix(2)
    feat_copy(1, 2).start()
    serve_b(gather_out, 3, 1, 2)
    mix(3)
    feat_copy(1, 3).start()
    serve_b(gather_out, 3, 2, 3)
    filter_taps(0)
    fconv[f] = sconv[0]
    serve_b(gather_out, 3, 3, 4)

    for i in range(1, FS):
        feat_wait(0, fs_of(i))

    total = jnp.zeros((TOK, 1), F32)
    for k in range(FS):
        values = jnp.concatenate(
            [fconv[k, other_half], fconv[k, own_half]], axis=0
        ).astype(F32)
        values = values + bias_ref[:, k * 128 : (k + 1) * 128]
        cvals[:, k * 128 : (k + 1) * 128] = values
        total = total + jnp.sum(values, axis=-1, keepdims=True)
    here = total / 512.0
    around = jnp.zeros((TOK, 1), F32)
    for k in range(FS):
        centred = cvals[:, k * 128 : (k + 1) * 128] - here
        around = around + jnp.sum(centred * centred, axis=-1, keepdims=True)
    stat_out[...] = jnp.where(lanes < 64, here, around)
    stat_copy = pltpu.make_async_remote_copy(
        src_ref=stat_out,
        dst_ref=stat_in,
        send_sem=stat_sent,
        recv_sem=stat_recv.at[0],
        device_id={"tp": partner},
        device_id_type=MESH,
    )
    stat_copy.start()
    mix(0)
    fatt[f] = satt[0]
    stat_copy.wait_recv()
    swapped = jnp.concatenate([stat_in[HALF:TOK, :], stat_in[0:HALF, :]], axis=0)
    there = swapped[:, 0:1]
    gap = here - there
    centre = 0.5 * (here + there)
    spread = (around + swapped[:, 64:65] + 256.0 * gap * gap) / 1024.0
    scale = lax.rsqrt(spread + EPSILON)
    for k in range(FS):
        at = slice(k * 128, (k + 1) * 128)
        v = (cvals[:, at] - centre) * scale * cgain_ref[:, at] + cshift_ref[:, at]
        raw[:, k * 256 + 128 : (k + 1) * 256] = (v / (1.0 + jnp.exp(-v))).astype(BF16)

    for i in range(1, FS):
        feat_wait(1, fs_of(i))
    for k in range(FS):
        raw[0:HALF, k * 256 : k * 256 + 128] = fatt[k, other_half]
        raw[HALF:TOK, k * 256 : k * 256 + 128] = fatt[k, own_half]

    serve_b(gather_out, 4, 0, 4)

    def part_copy(n):
        return pltpu.make_async_remote_copy(
            src_ref=part_out.at[n],
            dst_ref=part_in.at[n],
            send_sem=part_sent,
            recv_sem=part_recv.at[n],
            device_id={"tp": partner},
            device_id_type=MESH,
        )

    for n in range(D // CHUNK):
        weights = wout[n * CHUNK : (n + 1) * CHUNK, :]
        product = lax.dot_general(raw[...], weights, NT, preferred_element_type=F32)
        part_out[n] = product[0:HALF].astype(BF16)
        part_copy(n).start()
        part[n] = product[HALF:TOK]
    for n in range(D // CHUNK):
        part_copy(n).wait_recv()
        out_ref[:, n * CHUNK : (n + 1) * CHUNK] = (part[n] + part_in[n].astype(F32)).astype(BF16)

    def drain(ref, sent):
        pltpu.make_async_remote_copy(
            src_ref=ref,
            dst_ref=ref,
            send_sem=sent,
            recv_sem=stat_recv.at[0],
            device_id={"tp": partner},
            device_id_type=MESH,
        ).wait_send()

    drain(part_out, part_sent)
    stat_copy.wait_send()
    drain(sconv.at[1:FS], conv_sent)
    drain(satt.at[1:FS], att_sent)

    @pl.when(has_low)
    def _():
        drain(kvg.at[:, 0:144], halo_sent[0])

    @pl.when(has_high)
    def _():
        drain(kvg.at[:, 144:288], halo_sent[1])

    drain(tok.at[0:3], tok_sent)
    end_gather(gather_in)
    end_gather(gather_out)


def local(
    tokens,
    norm_gain,
    w_query,
    w_key,
    w_value,
    w_conv_in,
    w_conv_gate,
    sink_logit,
    conv_taps,
    conv_bias,
    channel_gain,
    channel_shift,
    w_attn_out,
    w_conv_out,
):
    vmem = pl.BlockSpec(memory_space=pltpu.VMEM)
    anywhere = pl.BlockSpec(memory_space=pl.ANY)
    dma = pltpu.SemaphoreType.DMA
    args = (
        tokens,
        norm_gain.reshape(1, -1),
        w_query,
        w_key,
        w_value,
        w_conv_in,
        w_conv_gate,
        sink_logit.reshape(1, -1),
        conv_taps,
        conv_bias.reshape(1, -1),
        channel_gain.reshape(1, -1),
        channel_shift.reshape(1, -1),
        w_attn_out.T,
        w_conv_out.T,
    )
    return pl.pallas_call(
        kernel,
        out_shape=jax.ShapeDtypeStruct((HALF, D), BF16),
        in_specs=[anywhere] * len(args),
        out_specs=vmem,
        scratch_shapes=[pltpu.VMEM(a.shape, a.dtype) for a in args]
        + [
            pltpu.VMEM((FS, TOK, D), BF16),
            pltpu.VMEM((D, 512), BF16),
            pltpu.VMEM((D, 1024), BF16),
            pltpu.VMEM((TOK, 128), F32),
            pltpu.VMEM((TOK, 128), F32),
            pltpu.VMEM((FS, 2, TOK, 128), BF16),
            pltpu.VMEM((FS, 288, 128), BF16),
            pltpu.VMEM((FS, 288, 128), F32),
            pltpu.VMEM((FS, 144, 128), BF16),
            pltpu.VMEM((FS, 144, 128), BF16),
            pltpu.VMEM((FS, TOK, 128), BF16),
            pltpu.VMEM((FS, TOK, 128), BF16),
            pltpu.VMEM((FS, TOK, 128), BF16),
            pltpu.VMEM((FS, TOK, 128), BF16),
            pltpu.VMEM((TOK, 1024), BF16),
            pltpu.VMEM((TOK, 512), F32),
            pltpu.VMEM((TOK, 128), F32),
            pltpu.VMEM((TOK, 128), F32),
            pltpu.VMEM((D // CHUNK, HALF, CHUNK), F32),
            pltpu.VMEM((D // CHUNK, HALF, CHUNK), BF16),
            pltpu.VMEM((D // CHUNK, HALF, CHUNK), BF16),
            dma((15,)),
            dma((RING,)),
            dma((RING, 4)),
            dma((RING,)),
            dma((RING, 4)),
            dma((FS, 2, 2)),
            dma((FS, 2)),
            dma((2, FS)),
            dma((1,)),
            dma((D // CHUNK,)),
            dma((9,)),
        ],
        compiler_params=pltpu.CompilerParams(
            collective_id=0, has_side_effects=True, vmem_limit_bytes=32 * 1024 * 1024
        ),
        name="fused",
    )(*(pltpu.with_memory_space_constraint(a, pltpu.HBM) for a in args))


def solution(mesh):
    in_specs = (
        P(("fs", "sp"), None),
        P(),
        P("sp", "tp"),
        P("sp", "tp"),
        P("sp", "tp"),
        P("sp", "tp"),
        P("sp", "tp"),
        P("tp"),
        P(None, "tp"),
        P("tp"),
        P("tp"),
        P("tp"),
        P(None, "sp"),
        P(None, "sp"),
    )
    out_specs = P(("fs", "sp", "tp"), None)
    return jax.shard_map(local, mesh=mesh, in_specs=in_specs, out_specs=out_specs, check_vma=False)
```

```python
import functools
import math

import jax
import jax.numpy as jnp
from jax import lax
from jax.experimental import pallas as pl
from jax.experimental.pallas import tpu as pltpu
from jax.sharding import PartitionSpec as P

HEAD_DIM = 64
WINDOW = 128
EPSILON = 1e-06
NEGATIVE = -1e30
ROPE_BASE = 10000.0
TOK = 256
HALF = 128
D = 2048
TAPS = 31
RING = 8
FS = 4
CHUNK = 1024
MESH = pl.DeviceIdType.MESH
NT = (((1,), (1,)), ((), ()))
F32 = jnp.float32
BF16 = jnp.bfloat16


def kernel(*refs):
    (
        tokens_hbm,
        gain_hbm,
        wq_hbm,
        wk_hbm,
        wv_hbm,
        wc_hbm,
        wg_hbm,
        sink_hbm,
        taps_hbm,
        bias_hbm,
        cgain_hbm,
        cshift_hbm,
        wao_hbm,
        wco_hbm,
        out_ref,
        tokens_ref,
        gain_ref,
        wq_ref,
        wk_ref,
        wv_ref,
        wc_ref,
        wg_ref,
        sink_ref,
        taps_ref,
        bias_ref,
        cgain_ref,
        cshift_ref,
        wao_ref,
        wco_ref,
        tok,
        win,
        wout,
        ctab,
        stab,
        qbuf,
        kvg,
        gext,
        low,
        high,
        sconv,
        satt,
        fconv,
        fatt,
        raw,
        cvals,
        stat_out,
        stat_in,
        part,
        part_out,
        part_in,
        load_sem,
        in_recv_a,
        in_recv_b,
        out_recv_a,
        out_recv_b,
        tok_recv,
        halo_recv,
        feat_recv,
        stat_recv,
        part_recv,
        send_sem,
    ) = refs
    in_sent, out_sent, tok_sent, conv_sent, att_sent, stat_sent, part_sent = (
        send_sem.at[k] for k in range(7)
    )
    halo_sent = (send_sem.at[7], send_sem.at[8])
    sp = lax.axis_index("sp")
    f = lax.axis_index("fs")
    c = lax.axis_index("tp")
    z, y = sp // RING, sp % RING
    me_a = (1 - c) * y + c * z
    me_b = (1 - c) * z + c * y
    partner = 1 - c

    def sp_of(a, b):
        return (1 - c) * (b * RING + a) + c * (a * RING + b)

    def wrap(v):
        return (v + 2 * RING) % RING

    def fs_of(step):
        return (f + step) % FS

    def load(k, src, dst):
        copy = pltpu.make_async_copy(src, dst, load_sem.at[k])
        copy.start()
        return copy

    own_half = pl.ds(pl.multiple_of(c * HALF, HALF), HALF)
    other_half = pl.ds(pl.multiple_of(partner * HALF, HALF), HALF)
    load_weights = [
        load(0, wq_hbm, wq_ref),
        load(1, wk_hbm, wk_ref),
        load(2, wv_hbm, wv_ref),
        load(3, wc_hbm, wc_ref),
        load(4, wg_hbm, wg_ref),
    ]
    load_own = [
        load(5, gain_hbm, gain_ref),
        load(6, tokens_hbm.at[own_half], tokens_ref.at[own_half]),
    ]
    load_other = load(7, tokens_hbm.at[other_half], tokens_ref.at[other_half])
    load_out = [load(8, wao_hbm, wao_ref), load(9, wco_hbm, wco_ref)]
    load_rest = [
        load(10, sink_hbm, sink_ref),
        load(11, taps_hbm, taps_ref),
        load(12, bias_hbm, bias_ref),
        load(13, cgain_hbm, cgain_ref),
        load(14, cshift_hbm, cshift_ref),
    ]

    has_low = sp > 0
    has_high = sp < RING * RING - 1

    barrier = pltpu.get_barrier_semaphore()

    def greet(**where):
        pl.semaphore_signal(barrier, inc=1, device_id=where, device_id_type=MESH)

    for step in range(1, RING):
        greet(sp=sp_of(wrap(me_a + step), me_b))
    greet(sp=sp_of(me_a, wrap(me_b + 1)))
    greet(sp=sp_of(me_a, wrap(me_b - 1)))
    for step in range(1, FS):
        greet(fs=fs_of(step))
    greet(tp=partner)

    greet(sp=(sp + 1) % (RING * RING))
    greet(sp=(sp + RING * RING - 1) % (RING * RING))

    lane32 = lax.broadcasted_iota(jnp.int32, (32, 128), 1)
    mine = pl.multiple_of(sp * 32, 32)
    cols = pl.ds(pl.multiple_of(f * 128, 128), 128)
    upper = f // 2
    for copy in load_weights:
        copy.wait()
    wk = wk_ref[...].astype(F32)
    wv = wv_ref[...].astype(F32)
    pick = (lane32 * 0 + upper) > 0
    wk = jnp.where(pick, pltpu.roll(wk, 64, 1), wk)
    wv = jnp.where(pick, wv, pltpu.roll(wv, 64, 1))
    win[pl.ds(mine, 32), 0:128] = wq_ref[:, cols]
    win[pl.ds(mine, 32), 128:256] = jnp.where(lane32 < 64, wk, wv).astype(BF16)
    win[pl.ds(mine, 32), 256:384] = wc_ref[:, cols]
    win[pl.ds(mine, 32), 384:512] = wg_ref[:, cols]

    def norm_rows(start):
        def body(i, carry):
            rows = pl.ds(pl.multiple_of(start + i * 16, 16), 16)
            x = tokens_ref[rows, :].astype(F32)
            scale = lax.rsqrt(jnp.mean(x * x, axis=-1, keepdims=True) + EPSILON)
            tok[f, rows, :] = (x * scale * gain_ref[...]).astype(BF16)
            return carry

        lax.fori_loop(0, HALF // 16, body, 0)

    pl.semaphore_wait(barrier, RING - 1 + 2 + FS - 1 + 1 + 2)

    def tok_rows(half, piece):
        return pl.ds(pl.multiple_of(half * HALF + piece * 64, 64), 64)

    def tok_copy(slot, half, piece, **where):
        ref = tok.at[slot, tok_rows(half, piece)]
        return pltpu.make_async_remote_copy(
            src_ref=ref,
            dst_ref=ref,
            send_sem=tok_sent,
            recv_sem=tok_recv.at[slot, half, piece],
            device_id=where,
            device_id_type=MESH,
        )

    def tok_first(direction, piece):
        return tok_copy(f, c, piece, fs=fs_of(1 + 2 * direction))

    def tok_second(direction):
        slot = fs_of(3 - 2 * direction)
        return tok_copy(slot, c, direction, fs=fs_of(1 + 2 * direction))

    def tok_to_pair(slot, piece):
        return tok_copy(slot, c, piece, tp=partner)

    def slab(buf, index):
        return buf.at[pl.ds(pl.multiple_of(index * 32, 32), 32)]

    def slab_copy(buf, recv, sent, index, target):
        ref = slab(buf, index)
        return pltpu.make_async_remote_copy(
            src_ref=ref,
            dst_ref=ref,
            send_sem=sent,
            recv_sem=recv,
            device_id={"sp": target},
            device_id_type=MESH,
        )

    def a_copy(gather, a, step):
        buf, recv_a, _, sent = gather
        target = sp_of(wrap(me_a + step), me_b)
        return slab_copy(buf, recv_a.at[a], sent, sp_of(a, me_b), target)

    def b_copy(gather, direction, j, b):
        buf, _, recv_b, sent = gather
        target = sp_of(me_a, wrap(me_b + 1 - 2 * direction))
        return slab_copy(buf, recv_b.at[b, j // 2], sent, sp_of(near(j), b), target)

    def wait_pair_of_slabs(gather, pair, b):
        buf, _, recv_b, sent = gather
        ref = buf.at[0:64]
        pltpu.make_async_remote_copy(
            src_ref=ref,
            dst_ref=ref,
            send_sem=sent,
            recv_sem=recv_b.at[b, pair],
            device_id={"tp": partner},
            device_id_type=MESH,
        ).wait_recv()

    def near(j):
        odd = j % 2
        dist = (j + 1) // 2
        return wrap(me_a + odd * dist - (1 - odd) * dist)

    def start_gather(gather, relay):
        b_copy(gather, 0, 0, me_b).start()
        b_copy(gather, 1, 0, me_b).start()

        if relay:
            a_copy(gather, me_a, 1).start()
            a_copy(gather, me_a, -1).start()
        else:
            for step in (1, -1, 4, 3, -3, 2, -2):
                a_copy(gather, me_a, step).start()

    def serve_a(gather, first, last, relay):
        def body(j, carry):
            a = near(j)
            a_copy(gather, a, 1).wait_recv()
            b_copy(gather, 0, j, me_b).start()
            b_copy(gather, 1, j, me_b).start()
            if relay:

                @pl.when(j % 2 == 0)
                def _():
                    a_copy(gather, a, 1).start()

                @pl.when((j % 2 == 1) & (j < 5))
                def _():
                    a_copy(gather, a, -1).start()

            return carry

        lax.fori_loop(first, last, body, 0)

    def serve_b(gather, step, first, last):
        def body(pair, carry):
            for direction in range(2):
                b = wrap(me_b - step if direction == 0 else me_b + step)
                wait_pair_of_slabs(gather, pair, b)

                def forward(b=b, direction=direction):
                    b_copy(gather, direction, 2 * pair, b).start()
                    b_copy(gather, direction, 2 * pair + 1, b).start()

                if step < 3:
                    forward()
                else:
                    pl.when(pair < 2 if direction == 0 else pair >= 2)(forward)
            return carry

        def body_last(pair, carry):
            wait_pair_of_slabs(gather, pair, wrap(me_b + step))
            return carry

        lax.fori_loop(first, last, body if step < 4 else body_last, 0)

    def end_gather(gather):
        buf, _, _, sent = gather
        ref = buf.at[0 : 63 * 32]
        pltpu.make_async_remote_copy(
            src_ref=ref,
            dst_ref=ref,
            send_sem=sent,
            recv_sem=stat_recv.at[0],
            device_id={"tp": partner},
            device_id_type=MESH,
        ).wait_send()

    gather_in = (win, in_recv_a, in_recv_b, in_sent)
    gather_out = (wout, out_recv_a, out_recv_b, out_sent)
    start_gather(gather_in, False)
    for copy in load_out:
        copy.wait()
    for k in range(FS):
        at = pl.ds(pl.multiple_of(c * 512 + k * 128, 128), 128)
        wout[pl.ds(mine, 32), k * 256 : k * 256 + 128] = wao_ref[:, at]
        wout[pl.ds(mine, 32), k * 256 + 128 : (k + 1) * 256] = wco_ref[:, at]

    start_gather(gather_out, True)
    for copy in load_own:
        copy.wait()
    norm_rows(pl.multiple_of(c * HALF, HALF))
    for first in range(2):
        for direction in range(2):
            tok_first(direction, (first + direction) % 2).start()

    load_other.wait()
    norm_rows(pl.multiple_of(partner * HALF, HALF))
    lane = lax.broadcasted_iota(jnp.int32, (HALF, 128), 1)
    frequency = jnp.exp((lane % 16).astype(F32) * (-math.log(ROPE_BASE) / 16))
    for k in range(2):
        token = lax.broadcasted_iota(jnp.int32, (HALF, 128), 0) + k * HALF
        place = jnp.where(lane % 64 < 32, sp * 4 + token // 64, token % 64)
        angle = place.astype(F32) * frequency
        ctab[k * HALF : (k + 1) * HALF, :] = jnp.cos(angle)
        sine = jnp.sin(angle)
        stab[k * HALF : (k + 1) * HALF, :] = jnp.where(lane % 32 < 16, -sine, sine)

    @pl.when(sp == 0)
    def _():
        low[...] = jnp.zeros_like(low)

    @pl.when(sp == RING * RING - 1)
    def _():
        high[...] = jnp.zeros_like(high)

    serve_a(gather_in, 1, 8, False)
    serve_a(gather_out, 1, 3, True)
    serve_b(gather_in, 1, 0, 4)

    serve_a(gather_out, 3, 5, True)
    serve_b(gather_in, 2, 0, 4)
    serve_a(gather_out, 5, 7, True)

    for direction in range(2):
        slot = fs_of(3 - 2 * direction)
        tok_to_pair(slot, direction).wait_recv()
        tok_second(direction).start()
        tok_to_pair(slot, direction).start()

    serve_b(gather_in, 3, 0, 4)
    serve_a(gather_out, 7, 8, True)

    for direction in range(2):
        slot = fs_of(3 - 2 * direction)
        tok_to_pair(slot, 1 - direction).wait_recv()
        tok_to_pair(slot, 1 - direction).start()

    serve_b(gather_out, 1, 0, 3)
    for piece in range(2):
        tok_to_pair(fs_of(2), piece).wait_recv()
        tok_to_pair(fs_of(2), piece).start()
    serve_b(gather_in, 4, 0, 4)
    for copy in load_rest:
        copy.wait()

    def halo_copy(i, side):
        at = side * 144
        return pltpu.make_async_remote_copy(
            src_ref=kvg.at[i, at : at + 144],
            dst_ref=(low if side else high).at[i],
            send_sem=halo_sent[side],
            recv_sem=halo_recv.at[i, side],
            device_id={"sp": sp + 2 * side - 1},
            device_id_type=MESH,
        )

    lanes = lax.broadcasted_iota(jnp.int32, (TOK, 128), 1)

    def rotated(x, cosine, sine):
        other = jnp.where(lanes % 32 < 16, pltpu.roll(x, 112, 1), pltpu.roll(x, 16, 1))
        return x * cosine + other * sine

    def project(i):
        slot = fs_of(i)
        acc = jnp.dot(tok[slot], win[...], preferred_element_type=F32)
        cosine, sine = ctab[...], stab[...]
        query = rotated(acc[:, 0:128], cosine, sine).astype(BF16).astype(F32) * HEAD_DIM**-0.5
        for h in range(2):
            head = query if h == 0 else pltpu.roll(query, 64, 1)
            head = jnp.where(lanes < 64, head, 0.0).astype(BF16)
            for block in range(2):
                qbuf[i, block, h * HALF : (h + 1) * HALF] = head[block * HALF : (block + 1) * HALF]
        pair = acc[:, 128:256]
        turned = rotated(pair, cosine, sine)
        kvg[i, 16:272] = jnp.where(lanes < 64, turned, pair).astype(BF16)
        glu = (acc[:, 256:384] * jax.nn.sigmoid(acc[:, 384:512])).astype(BF16)
        kvg[i, 0:16] = glu[0:16]
        kvg[i, 272:288] = glu[240:256]
        gext[i, 16:272] = glu.astype(F32)

        @pl.when(has_low)
        def _():
            halo_copy(i, 0).start()

        @pl.when(has_high)
        def _():
            halo_copy(i, 1).start()

    row_at = lax.broadcasted_iota(jnp.int32, (TOK, TOK), 0) % HALF
    key_at = lax.broadcasted_iota(jnp.int32, (TOK, TOK), 1)
    half_row = lax.broadcasted_iota(jnp.int32, (TOK, HALF), 0) % HALF
    half_key = lax.broadcasted_iota(jnp.int32, (TOK, HALF), 1)
    half_lane = lax.broadcasted_iota(jnp.int32, (HALF, 128), 1)
    far = RING * TOK
    own_valid = (key_at - row_at <= WINDOW, key_at >= row_at)
    halo_valid = (
        half_key >= half_row + jnp.where(has_low, 0, far),
        half_key + jnp.where(has_high, 0, far) <= half_row,
    )
    head_lane = lax.broadcasted_iota(jnp.int32, (1, 8), 1)
    sinks = [
        jnp.sum(jnp.where(head_lane == 2 * f + h, sink_ref[...], 0.0), axis=-1, keepdims=True)
        for h in range(2)
    ]
    first_head = lax.broadcasted_iota(jnp.int32, (TOK, 1), 0) < HALF
    sink = jnp.where(first_head, sinks[0], sinks[1])

    def mix(i):
        own_kv = kvg[i, 16:272]
        own_ones = jnp.where(lanes < 64, jnp.ones_like(own_kv), own_kv)
        for block in range(2):
            near_kv = low[i, 0:128] if block == 0 else high[i, 16:144]
            near_ones = jnp.where(half_lane < 64, jnp.ones_like(near_kv), near_kv)
            q = qbuf[i, block]
            s_own = lax.dot_general(q, own_kv, NT, preferred_element_type=F32)
            s_near = lax.dot_general(q, near_kv, NT, preferred_element_type=F32)
            s_own = jnp.where(own_valid[block], s_own, NEGATIVE)
            s_near = jnp.where(halo_valid[block], s_near, NEGATIVE)
            top = jnp.maximum(jnp.maximum(s_own[:, 0:128], s_own[:, 128:256]), s_near)
            top = jnp.maximum(jnp.max(top, axis=-1, keepdims=True), sink)
            p_own = jnp.exp(s_own - top).astype(BF16)
            p_near = jnp.exp(s_near - top).astype(BF16)
            mixed = jnp.dot(p_own, own_ones, preferred_element_type=F32) + jnp.dot(
                p_near, near_ones, preferred_element_type=F32
            )
            mixed = mixed / (pltpu.roll(mixed, 64, 1) + jnp.exp(sink - top))
            joined = jnp.where(half_lane < 64, pltpu.roll(mixed[0:HALF], 64, 1), mixed[HALF:TOK])
            satt[i, block * HALF : (block + 1) * HALF] = joined.astype(BF16)

    def filter_taps(i):
        @pl.when(has_low)
        def _():
            halo_copy(i, 1).wait_recv()

        @pl.when(has_high)
        def _():
            halo_copy(i, 0).wait_recv()

        gext[i, 0:16] = low[i, 128:144].astype(F32)
        gext[i, 272:288] = high[i, 0:16].astype(F32)

        for block in range(4):
            total = jnp.zeros((64, 128), F32)
            for k in range(TAPS):
                at = block * 64 + k + 1
                total = total + taps_ref[k : k + 1, cols] * gext[i, at : at + 64]
            sconv[i, block * 64 : (block + 1) * 64] = total.astype(BF16)

    def feat_copy(kind, i):
        return pltpu.make_async_remote_copy(
            src_ref=(sconv, satt)[kind].at[i],
            dst_ref=(fconv, fatt)[kind].at[f],
            send_sem=(conv_sent, att_sent)[kind],
            recv_sem=feat_recv.at[kind, f],
            device_id={"fs": fs_of(i)},
            device_id_type=MESH,
        )

    def feat_wait(kind, src):
        pltpu.make_async_remote_copy(
            src_ref=(sconv, satt)[kind].at[0],
            dst_ref=(fconv, fatt)[kind].at[src],
            send_sem=(conv_sent, att_sent)[kind],
            recv_sem=feat_recv.at[kind, src],
            device_id={"tp": partner},
            device_id_type=MESH,
        ).wait_recv()

    def wait_pair(slot):
        tok_copy(slot, partner, 0, tp=partner).wait_recv()
        tok_copy(slot, partner, 1, tp=partner).wait_recv()

    wait_pair(fs_of(1))
    project(1)
    serve_b(gather_out, 1, 3, 4)
    wait_pair(fs_of(3))
    project(3)
    wait_pair(fs_of(2))
    project(2)
    serve_b(gather_out, 2, 0, 1)
    project(0)
    serve_b(gather_out, 2, 1, 4)
    filter_taps(1)
    feat_copy(0, 1).start()
    filter_taps(3)
    feat_copy(0, 3).start()
    mix(1)
    feat_copy(1, 1).start()
    serve_b(gather_out, 3, 0, 1)
    filter_taps(2)
    feat_copy(0, 2).start()
    mix(2)
    feat_copy(1, 2).start()
    serve_b(gather_out, 3, 1, 2)
    mix(3)
    feat_copy(1, 3).start()
    serve_b(gather_out, 3, 2, 3)
    filter_taps(0)
    fconv[f] = sconv[0]
    serve_b(gather_out, 3, 3, 4)

    for i in range(1, FS):
        feat_wait(0, fs_of(i))

    total = jnp.zeros((TOK, 1), F32)
    for k in range(FS):
        values = jnp.concatenate(
            [fconv[k, other_half], fconv[k, own_half]], axis=0
        ).astype(F32)
        values = values + bias_ref[:, k * 128 : (k + 1) * 128]
        cvals[:, k * 128 : (k + 1) * 128] = values
        total = total + jnp.sum(values, axis=-1, keepdims=True)
    here = total / 512.0
    around = jnp.zeros((TOK, 1), F32)
    for k in range(FS):
        centred = cvals[:, k * 128 : (k + 1) * 128] - here
        around = around + jnp.sum(centred * centred, axis=-1, keepdims=True)
    stat_out[...] = jnp.where(lanes < 64, here, around)
    stat_copy = pltpu.make_async_remote_copy(
        src_ref=stat_out,
        dst_ref=stat_in,
        send_sem=stat_sent,
        recv_sem=stat_recv.at[0],
        device_id={"tp": partner},
        device_id_type=MESH,
    )
    stat_copy.start()
    mix(0)
    fatt[f] = satt[0]
    stat_copy.wait_recv()
    swapped = jnp.concatenate([stat_in[HALF:TOK, :], stat_in[0:HALF, :]], axis=0)
    there = swapped[:, 0:1]
    gap = here - there
    centre = 0.5 * (here + there)
    spread = (around + swapped[:, 64:65] + 256.0 * gap * gap) / 1024.0
    scale = lax.rsqrt(spread + EPSILON)
    for k in range(FS):
        at = slice(k * 128, (k + 1) * 128)
        v = (cvals[:, at] - centre) * scale * cgain_ref[:, at] + cshift_ref[:, at]
        raw[:, k * 256 + 128 : (k + 1) * 256] = (v / (1.0 + jnp.exp(-v))).astype(BF16)

    for i in range(1, FS):
        feat_wait(1, fs_of(i))
    for k in range(FS):
        raw[0:HALF, k * 256 : k * 256 + 128] = fatt[k, other_half]
        raw[HALF:TOK, k * 256 : k * 256 + 128] = fatt[k, own_half]

    serve_b(gather_out, 4, 0, 4)

    def part_copy(n):
        return pltpu.make_async_remote_copy(
            src_ref=part_out.at[n],
            dst_ref=part_in.at[n],
            send_sem=part_sent,
            recv_sem=part_recv.at[n],
            device_id={"tp": partner},
            device_id_type=MESH,
        )

    for n in range(D // CHUNK):
        weights = wout[n * CHUNK : (n + 1) * CHUNK, :]
        product = lax.dot_general(raw[...], weights, NT, preferred_element_type=F32)
        part_out[n] = product[0:HALF].astype(BF16)
        part_copy(n).start()
        part[n] = product[HALF:TOK]
    for n in range(D // CHUNK):
        part_copy(n).wait_recv()
        out_ref[:, n * CHUNK : (n + 1) * CHUNK] = (part[n] + part_in[n].astype(F32)).astype(BF16)

    def drain(ref, sent):
        pltpu.make_async_remote_copy(
            src_ref=ref,
            dst_ref=ref,
            send_sem=sent,
            recv_sem=stat_recv.at[0],
            device_id={"tp": partner},
            device_id_type=MESH,
        ).wait_send()

    drain(part_out, part_sent)
    stat_copy.wait_send()
    drain(sconv.at[1:FS], conv_sent)
    drain(satt.at[1:FS], att_sent)

    @pl.when(has_low)
    def _():
        drain(kvg.at[:, 0:144], halo_sent[0])

    @pl.when(has_high)
    def _():
        drain(kvg.at[:, 144:288], halo_sent[1])

    drain(tok.at[0:3], tok_sent)
    end_gather(gather_in)
    end_gather(gather_out)


def local(
    tokens,
    norm_gain,
    w_query,
    w_key,
    w_value,
    w_conv_in,
    w_conv_gate,
    sink_logit,
    conv_taps,
    conv_bias,
    channel_gain,
    channel_shift,
    w_attn_out,
    w_conv_out,
):
    vmem = pl.BlockSpec(memory_space=pltpu.VMEM)
    anywhere = pl.BlockSpec(memory_space=pl.ANY)
    dma = pltpu.SemaphoreType.DMA
    args = (
        tokens,
        norm_gain.reshape(1, -1),
        w_query,
        w_key,
        w_value,
        w_conv_in,
        w_conv_gate,
        sink_logit.reshape(1, -1),
        conv_taps,
        conv_bias.reshape(1, -1),
        channel_gain.reshape(1, -1),
        channel_shift.reshape(1, -1),
        w_attn_out.T,
        w_conv_out.T,
    )
    return pl.pallas_call(
        kernel,
        out_shape=jax.ShapeDtypeStruct((HALF, D), BF16),
        in_specs=[anywhere] * len(args),
        out_specs=vmem,
        scratch_shapes=[pltpu.VMEM(a.shape, a.dtype) for a in args]
        + [
            pltpu.VMEM((FS, TOK, D), BF16),
            pltpu.VMEM((D, 512), BF16),
            pltpu.VMEM((D, 1024), BF16),
            pltpu.VMEM((TOK, 128), F32),
            pltpu.VMEM((TOK, 128), F32),
            pltpu.VMEM((FS, 2, TOK, 128), BF16),
            pltpu.VMEM((FS, 288, 128), BF16),
            pltpu.VMEM((FS, 288, 128), F32),
            pltpu.VMEM((FS, 144, 128), BF16),
            pltpu.VMEM((FS, 144, 128), BF16),
            pltpu.VMEM((FS, TOK, 128), BF16),
            pltpu.VMEM((FS, TOK, 128), BF16),
            pltpu.VMEM((FS, TOK, 128), BF16),
            pltpu.VMEM((FS, TOK, 128), BF16),
            pltpu.VMEM((TOK, 1024), BF16),
            pltpu.VMEM((TOK, 512), F32),
            pltpu.VMEM((TOK, 128), F32),
            pltpu.VMEM((TOK, 128), F32),
            pltpu.VMEM((D // CHUNK, HALF, CHUNK), F32),
            pltpu.VMEM((D // CHUNK, HALF, CHUNK), BF16),
            pltpu.VMEM((D // CHUNK, HALF, CHUNK), BF16),
            dma((15,)),
            dma((RING,)),
            dma((RING, 4)),
            dma((RING,)),
            dma((RING, 4)),
            dma((FS, 2, 2)),
            dma((FS, 2)),
            dma((2, FS)),
            dma((1,)),
            dma((D // CHUNK,)),
            dma((9,)),
        ],
        compiler_params=pltpu.CompilerParams(
            collective_id=0, has_side_effects=True, vmem_limit_bytes=32 * 1024 * 1024
        ),
        name="fused",
    )(*(pltpu.with_memory_space_constraint(a, pltpu.HBM) for a in args))


def solution(mesh):
    in_specs = (
        P(("fs", "sp"), None),
        P(),
        P("sp", "tp"),
        P("sp", "tp"),
        P("sp", "tp"),
        P("sp", "tp"),
        P("sp", "tp"),
        P("tp"),
        P(None, "tp"),
        P("tp"),
        P("tp"),
        P("tp"),
        P(None, "sp"),
        P(None, "sp"),
    )
    out_specs = P(("fs", "sp", "tp"), None)
    return jax.shard_map(local, mesh=mesh, in_specs=in_specs, out_specs=out_specs, check_vma=False)
```

```python
import functools
import math

import jax
import jax.numpy as jnp
from jax import lax
from jax.experimental import pallas as pl
from jax.experimental.pallas import tpu as pltpu
from jax.sharding import PartitionSpec as P

HEAD_DIM = 64
WINDOW = 128
EPSILON = 1e-06
NEGATIVE = -1e30
ROPE_BASE = 10000.0
TOK = 256
HALF = 128
D = 2048
TAPS = 31
RING = 8
FS = 4
CHUNK = 1024
MESH = pl.DeviceIdType.MESH
NT = (((1,), (1,)), ((), ()))
F32 = jnp.float32
BF16 = jnp.bfloat16


def kernel(*refs):
    (
        tokens_hbm,
        gain_hbm,
        wq_hbm,
        wk_hbm,
        wv_hbm,
        wc_hbm,
        wg_hbm,
        sink_hbm,
        taps_hbm,
        bias_hbm,
        cgain_hbm,
        cshift_hbm,
        wao_hbm,
        wco_hbm,
        out_ref,
        tokens_ref,
        gain_ref,
        wq_ref,
        wk_ref,
        wv_ref,
        wc_ref,
        wg_ref,
        sink_ref,
        taps_ref,
        bias_ref,
        cgain_ref,
        cshift_ref,
        wao_ref,
        wco_ref,
        tok,
        win,
        wout,
        ctab,
        stab,
        qbuf,
        kvg,
        gext,
        low,
        high,
        sconv,
        satt,
        fconv,
        fatt,
        raw,
        cvals,
        stat_out,
        stat_in,
        part,
        part_out,
        part_in,
        load_sem,
        in_recv_a,
        in_recv_b,
        out_recv_a,
        out_recv_b,
        tok_recv,
        halo_recv,
        feat_recv,
        stat_recv,
        part_recv,
        send_sem,
    ) = refs
    in_sent, out_sent, tok_sent, conv_sent, att_sent, stat_sent, part_sent = (
        send_sem.at[k] for k in range(7)
    )
    halo_sent = (send_sem.at[7], send_sem.at[8])
    sp = lax.axis_index("sp")
    f = lax.axis_index("fs")
    c = lax.axis_index("tp")
    z, y = sp // RING, sp % RING
    me_a = (1 - c) * y + c * z
    me_b = (1 - c) * z + c * y
    partner = 1 - c

    def sp_of(a, b):
        return (1 - c) * (b * RING + a) + c * (a * RING + b)

    def wrap(v):
        return (v + 2 * RING) % RING

    def fs_of(step):
        return (f + step) % FS

    def load(k, src, dst):
        copy = pltpu.make_async_copy(src, dst, load_sem.at[k])
        copy.start()
        return copy

    own_half = pl.ds(pl.multiple_of(c * HALF, HALF), HALF)
    other_half = pl.ds(pl.multiple_of(partner * HALF, HALF), HALF)
    load_weights = [
        load(0, wq_hbm, wq_ref),
        load(1, wk_hbm, wk_ref),
        load(2, wv_hbm, wv_ref),
        load(3, wc_hbm, wc_ref),
        load(4, wg_hbm, wg_ref),
    ]
    load_own = [
        load(5, gain_hbm, gain_ref),
        load(6, tokens_hbm.at[own_half], tokens_ref.at[own_half]),
    ]
    load_other = load(7, tokens_hbm.at[other_half], tokens_ref.at[other_half])
    load_out = [load(8, wao_hbm, wao_ref), load(9, wco_hbm, wco_ref)]
    load_rest = [
        load(10, sink_hbm, sink_ref),
        load(11, taps_hbm, taps_ref),
        load(12, bias_hbm, bias_ref),
        load(13, cgain_hbm, cgain_ref),
        load(14, cshift_hbm, cshift_ref),
    ]

    has_low = sp > 0
    has_high = sp < RING * RING - 1

    barrier = pltpu.get_barrier_semaphore()

    def greet(**where):
        pl.semaphore_signal(barrier, inc=1, device_id=where, device_id_type=MESH)

    for step in range(1, RING):
        greet(sp=sp_of(wrap(me_a + step), me_b))
    greet(sp=sp_of(me_a, wrap(me_b + 1)))
    greet(sp=sp_of(me_a, wrap(me_b - 1)))
    for step in range(1, FS):
        greet(fs=fs_of(step))
    greet(tp=partner)

    greet(sp=(sp + 1) % (RING * RING))
    greet(sp=(sp + RING * RING - 1) % (RING * RING))

    lane32 = lax.broadcasted_iota(jnp.int32, (32, 128), 1)
    mine = pl.multiple_of(sp * 32, 32)
    cols = pl.ds(pl.multiple_of(f * 128, 128), 128)
    upper = f // 2
    for copy in load_weights:
        copy.wait()
    wk = wk_ref[...].astype(F32)
    wv = wv_ref[...].astype(F32)
    pick = (lane32 * 0 + upper) > 0
    wk = jnp.where(pick, pltpu.roll(wk, 64, 1), wk)
    wv = jnp.where(pick, wv, pltpu.roll(wv, 64, 1))
    win[pl.ds(mine, 32), 0:128] = wq_ref[:, cols]
    win[pl.ds(mine, 32), 128:256] = jnp.where(lane32 < 64, wk, wv).astype(BF16)
    win[pl.ds(mine, 32), 256:384] = wc_ref[:, cols]
    win[pl.ds(mine, 32), 384:512] = wg_ref[:, cols]

    def norm_rows(start):
        def body(i, carry):
            rows = pl.ds(pl.multiple_of(start + i * 16, 16), 16)
            x = tokens_ref[rows, :].astype(F32)
            scale = lax.rsqrt(jnp.mean(x * x, axis=-1, keepdims=True) + EPSILON)
            tok[f, rows, :] = (x * scale * gain_ref[...]).astype(BF16)
            return carry

        lax.fori_loop(0, HALF // 16, body, 0)

    pl.semaphore_wait(barrier, RING - 1 + 2 + FS - 1 + 1 + 2)

    def tok_rows(half, piece):
        return pl.ds(pl.multiple_of(half * HALF + piece * 64, 64), 64)

    def tok_copy(slot, half, piece, **where):
        ref = tok.at[slot, tok_rows(half, piece)]
        return pltpu.make_async_remote_copy(
            src_ref=ref,
            dst_ref=ref,
            send_sem=tok_sent,
            recv_sem=tok_recv.at[slot, half, piece],
            device_id=where,
            device_id_type=MESH,
        )

    def tok_first(direction, piece):
        return tok_copy(f, c, piece, fs=fs_of(1 + 2 * direction))

    def tok_second(direction):
        slot = fs_of(3 - 2 * direction)
        return tok_copy(slot, c, direction, fs=fs_of(1 + 2 * direction))

    def tok_to_pair(slot, piece):
        return tok_copy(slot, c, piece, tp=partner)

    def slab(buf, index):
        return buf.at[pl.ds(pl.multiple_of(index * 32, 32), 32)]

    def slab_copy(buf, recv, sent, index, target):
        ref = slab(buf, index)
        return pltpu.make_async_remote_copy(
            src_ref=ref,
            dst_ref=ref,
            send_sem=sent,
            recv_sem=recv,
            device_id={"sp": target},
            device_id_type=MESH,
        )

    def a_copy(gather, a, step):
        buf, recv_a, _, sent = gather
        target = sp_of(wrap(me_a + step), me_b)
        return slab_copy(buf, recv_a.at[a], sent, sp_of(a, me_b), target)

    def b_copy(gather, direction, j, b):
        buf, _, recv_b, sent = gather
        target = sp_of(me_a, wrap(me_b + 1 - 2 * direction))
        return slab_copy(buf, recv_b.at[b, j // 2], sent, sp_of(near(j), b), target)

    def wait_pair_of_slabs(gather, pair, b):
        buf, _, recv_b, sent = gather
        ref = buf.at[0:64]
        pltpu.make_async_remote_copy(
            src_ref=ref,
            dst_ref=ref,
            send_sem=sent,
            recv_sem=recv_b.at[b, pair],
            device_id={"tp": partner},
            device_id_type=MESH,
        ).wait_recv()

    def near(j):
        odd = j % 2
        dist = (j + 1) // 2
        return wrap(me_a + odd * dist - (1 - odd) * dist)

    def start_gather(gather, relay):
        b_copy(gather, 0, 0, me_b).start()
        b_copy(gather, 1, 0, me_b).start()

        if relay:
            a_copy(gather, me_a, 1).start()
            a_copy(gather, me_a, -1).start()
        else:
            for step in (1, -1, 4, 3, -3, 2, -2):
                a_copy(gather, me_a, step).start()

    def serve_a(gather, first, last, relay):
        def body(j, carry):
            a = near(j)
            a_copy(gather, a, 1).wait_recv()
            b_copy(gather, 0, j, me_b).start()
            b_copy(gather, 1, j, me_b).start()
            if relay:

                @pl.when(j % 2 == 0)
                def _():
                    a_copy(gather, a, 1).start()

                @pl.when((j % 2 == 1) & (j < 5))
                def _():
                    a_copy(gather, a, -1).start()

            return carry

        lax.fori_loop(first, last, body, 0)

    def serve_b(gather, step, first, last):
        def body(pair, carry):
            for direction in range(2):
                b = wrap(me_b - step if direction == 0 else me_b + step)
                wait_pair_of_slabs(gather, pair, b)

                def forward(b=b, direction=direction):
                    b_copy(gather, direction, 2 * pair, b).start()
                    b_copy(gather, direction, 2 * pair + 1, b).start()

                if step < 3:
                    forward()
                else:
                    pl.when(pair < 2 if direction == 0 else pair >= 2)(forward)
            return carry

        def body_last(pair, carry):
            wait_pair_of_slabs(gather, pair, wrap(me_b + step))
            return carry

        lax.fori_loop(first, last, body if step < 4 else body_last, 0)

    def end_gather(gather):
        buf, _, _, sent = gather
        ref = buf.at[0 : 63 * 32]
        pltpu.make_async_remote_copy(
            src_ref=ref,
            dst_ref=ref,
            send_sem=sent,
            recv_sem=stat_recv.at[0],
            device_id={"tp": partner},
            device_id_type=MESH,
        ).wait_send()

    gather_in = (win, in_recv_a, in_recv_b, in_sent)
    gather_out = (wout, out_recv_a, out_recv_b, out_sent)
    start_gather(gather_in, False)
    for copy in load_out:
        copy.wait()
    for k in range(FS):
        at = pl.ds(pl.multiple_of(c * 512 + k * 128, 128), 128)
        wout[pl.ds(mine, 32), k * 256 : k * 256 + 128] = wao_ref[:, at]
        wout[pl.ds(mine, 32), k * 256 + 128 : (k + 1) * 256] = wco_ref[:, at]

    start_gather(gather_out, True)
    for copy in load_own:
        copy.wait()
    norm_rows(pl.multiple_of(c * HALF, HALF))
    for first in range(2):
        for direction in range(2):
            tok_first(direction, (first + direction) % 2).start()

    load_other.wait()
    norm_rows(pl.multiple_of(partner * HALF, HALF))
    lane = lax.broadcasted_iota(jnp.int32, (HALF, 128), 1)
    frequency = jnp.exp((lane % 16).astype(F32) * (-math.log(ROPE_BASE) / 16))
    for k in range(2):
        token = lax.broadcasted_iota(jnp.int32, (HALF, 128), 0) + k * HALF
        place = jnp.where(lane % 64 < 32, sp * 4 + token // 64, token % 64)
        angle = place.astype(F32) * frequency
        ctab[k * HALF : (k + 1) * HALF, :] = jnp.cos(angle)
        sine = jnp.sin(angle)
        stab[k * HALF : (k + 1) * HALF, :] = jnp.where(lane % 32 < 16, -sine, sine)

    @pl.when(sp == 0)
    def _():
        low[...] = jnp.zeros_like(low)

    @pl.when(sp == RING * RING - 1)
    def _():
        high[...] = jnp.zeros_like(high)

    serve_a(gather_in, 1, 8, False)
    serve_a(gather_out, 1, 3, True)
    serve_b(gather_in, 1, 0, 4)

    serve_a(gather_out, 3, 5, True)
    serve_b(gather_in, 2, 0, 4)
    serve_a(gather_out, 5, 7, True)

    for direction in range(2):
        slot = fs_of(3 - 2 * direction)
        tok_to_pair(slot, direction).wait_recv()
        tok_second(direction).start()
        tok_to_pair(slot, direction).start()

    serve_b(gather_in, 3, 0, 4)
    serve_a(gather_out, 7, 8, True)

    for direction in range(2):
        slot = fs_of(3 - 2 * direction)
        tok_to_pair(slot, 1 - direction).wait_recv()
        tok_to_pair(slot, 1 - direction).start()

    serve_b(gather_out, 1, 0, 3)
    for piece in range(2):
        tok_to_pair(fs_of(2), piece).wait_recv()
        tok_to_pair(fs_of(2), piece).start()
    serve_b(gather_in, 4, 0, 4)
    for copy in load_rest:
        copy.wait()

    def halo_copy(i, side):
        at = side * 144
        return pltpu.make_async_remote_copy(
            src_ref=kvg.at[i, at : at + 144],
            dst_ref=(low if side else high).at[i],
            send_sem=halo_sent[side],
            recv_sem=halo_recv.at[i, side],
            device_id={"sp": (sp + RING * RING + 2 * side - 1) % (RING * RING)},
            device_id_type=MESH,
        )

    lanes = lax.broadcasted_iota(jnp.int32, (TOK, 128), 1)

    def rotated(x, cosine, sine):
        other = jnp.where(lanes % 32 < 16, pltpu.roll(x, 112, 1), pltpu.roll(x, 16, 1))
        return x * cosine + other * sine

    def project(i):
        slot = fs_of(i)
        acc = jnp.dot(tok[slot], win[...], preferred_element_type=F32)
        cosine, sine = ctab[...], stab[...]
        query = rotated(acc[:, 0:128], cosine, sine).astype(BF16).astype(F32) * HEAD_DIM**-0.5
        for h in range(2):
            head = query if h == 0 else pltpu.roll(query, 64, 1)
            head = jnp.where(lanes < 64, head, 0.0).astype(BF16)
            for block in range(2):
                qbuf[i, block, h * HALF : (h + 1) * HALF] = head[block * HALF : (block + 1) * HALF]
        pair = acc[:, 128:256]
        turned = rotated(pair, cosine, sine)
        kvg[i, 16:272] = jnp.where(lanes < 64, turned, pair).astype(BF16)
        glu = (acc[:, 256:384] * jax.nn.sigmoid(acc[:, 384:512])).astype(BF16)
        kvg[i, 0:16] = glu[0:16]
        kvg[i, 272:288] = glu[240:256]
        gext[i, 16:272] = glu.astype(F32)

        @pl.when(has_low)
        def _():
            halo_copy(i, 0).start()

        @pl.when(has_high)
        def _():
            halo_copy(i, 1).start()

    row_at = lax.broadcasted_iota(jnp.int32, (TOK, TOK), 0) % HALF
    key_at = lax.broadcasted_iota(jnp.int32, (TOK, TOK), 1)
    half_row = lax.broadcasted_iota(jnp.int32, (TOK, HALF), 0) % HALF
    half_key = lax.broadcasted_iota(jnp.int32, (TOK, HALF), 1)
    half_lane = lax.broadcasted_iota(jnp.int32, (HALF, 128), 1)
    far = RING * TOK
    own_valid = (key_at - row_at <= WINDOW, key_at >= row_at)
    halo_valid = (
        half_key >= half_row + jnp.where(has_low, 0, far),
        half_key + jnp.where(has_high, 0, far) <= half_row,
    )
    head_lane = lax.broadcasted_iota(jnp.int32, (1, 8), 1)
    sinks = [
        jnp.sum(jnp.where(head_lane == 2 * f + h, sink_ref[...], 0.0), axis=-1, keepdims=True)
        for h in range(2)
    ]
    first_head = lax.broadcasted_iota(jnp.int32, (TOK, 1), 0) < HALF
    sink = jnp.where(first_head, sinks[0], sinks[1])

    def mix(i):
        own_kv = kvg[i, 16:272]
        own_ones = jnp.where(lanes < 64, jnp.ones_like(own_kv), own_kv)
        for block in range(2):
            near_kv = low[i, 0:128] if block == 0 else high[i, 16:144]
            near_ones = jnp.where(half_lane < 64, jnp.ones_like(near_kv), near_kv)
            q = qbuf[i, block]
            s_own = lax.dot_general(q, own_kv, NT, preferred_element_type=F32)
            s_near = lax.dot_general(q, near_kv, NT, preferred_element_type=F32)
            s_own = jnp.where(own_valid[block], s_own, NEGATIVE)
            s_near = jnp.where(halo_valid[block], s_near, NEGATIVE)
            top = jnp.maximum(jnp.maximum(s_own[:, 0:128], s_own[:, 128:256]), s_near)
            top = jnp.maximum(jnp.max(top, axis=-1, keepdims=True), sink)
            p_own = jnp.exp(s_own - top).astype(BF16)
            p_near = jnp.exp(s_near - top).astype(BF16)
            mixed = jnp.dot(p_own, own_ones, preferred_element_type=F32) + jnp.dot(
                p_near, near_ones, preferred_element_type=F32
            )
            mixed = mixed / (pltpu.roll(mixed, 64, 1) + jnp.exp(sink - top))
            joined = jnp.where(half_lane < 64, pltpu.roll(mixed[0:HALF], 64, 1), mixed[HALF:TOK])
            satt[i, block * HALF : (block + 1) * HALF] = joined.astype(BF16)

    def filter_taps(i):
        @pl.when(has_low)
        def _():
            halo_copy(i, 1).wait_recv()

        @pl.when(has_high)
        def _():
            halo_copy(i, 0).wait_recv()

        gext[i, 0:16] = low[i, 128:144].astype(F32)
        gext[i, 272:288] = high[i, 0:16].astype(F32)

        for block in range(4):
            total = jnp.zeros((64, 128), F32)
            for k in range(TAPS):
                at = block * 64 + k + 1
                total = total + taps_ref[k : k + 1, cols] * gext[i, at : at + 64]
            sconv[i, block * 64 : (block + 1) * 64] = total.astype(BF16)

    def feat_copy(kind, i):
        return pltpu.make_async_remote_copy(
            src_ref=(sconv, satt)[kind].at[i],
            dst_ref=(fconv, fatt)[kind].at[f],
            send_sem=(conv_sent, att_sent)[kind],
            recv_sem=feat_recv.at[kind, f],
            device_id={"fs": fs_of(i)},
            device_id_type=MESH,
        )

    def feat_wait(kind, src):
        pltpu.make_async_remote_copy(
            src_ref=(sconv, satt)[kind].at[0],
            dst_ref=(fconv, fatt)[kind].at[src],
            send_sem=(conv_sent, att_sent)[kind],
            recv_sem=feat_recv.at[kind, src],
            device_id={"tp": partner},
            device_id_type=MESH,
        ).wait_recv()

    def wait_pair(slot):
        tok_copy(slot, partner, 0, tp=partner).wait_recv()
        tok_copy(slot, partner, 1, tp=partner).wait_recv()

    wait_pair(fs_of(1))
    project(1)
    serve_b(gather_out, 1, 3, 4)
    wait_pair(fs_of(3))
    project(3)
    wait_pair(fs_of(2))
    project(2)
    serve_b(gather_out, 2, 0, 1)
    project(0)
    serve_b(gather_out, 2, 1, 4)
    filter_taps(1)
    feat_copy(0, 1).start()
    filter_taps(3)
    feat_copy(0, 3).start()
    mix(1)
    feat_copy(1, 1).start()
    serve_b(gather_out, 3, 0, 1)
    filter_taps(2)
    feat_copy(0, 2).start()
    mix(2)
    feat_copy(1, 2).start()
    serve_b(gather_out, 3, 1, 2)
    mix(3)
    feat_copy(1, 3).start()
    serve_b(gather_out, 3, 2, 3)
    filter_taps(0)
    fconv[f] = sconv[0]
    serve_b(gather_out, 3, 3, 4)

    for i in range(1, FS):
        feat_wait(0, fs_of(i))

    total = jnp.zeros((TOK, 1), F32)
    for k in range(FS):
        values = jnp.concatenate(
            [fconv[k, other_half], fconv[k, own_half]], axis=0
        ).astype(F32)
        values = values + bias_ref[:, k * 128 : (k + 1) * 128]
        cvals[:, k * 128 : (k + 1) * 128] = values
        total = total + jnp.sum(values, axis=-1, keepdims=True)
    here = total / 512.0
    around = jnp.zeros((TOK, 1), F32)
    for k in range(FS):
        centred = cvals[:, k * 128 : (k + 1) * 128] - here
        around = around + jnp.sum(centred * centred, axis=-1, keepdims=True)
    stat_out[...] = jnp.where(lanes < 64, here, around)
    stat_copy = pltpu.make_async_remote_copy(
        src_ref=stat_out,
        dst_ref=stat_in,
        send_sem=stat_sent,
        recv_sem=stat_recv.at[0],
        device_id={"tp": partner},
        device_id_type=MESH,
    )
    stat_copy.start()
    mix(0)
    fatt[f] = satt[0]
    stat_copy.wait_recv()
    swapped = jnp.concatenate([stat_in[HALF:TOK, :], stat_in[0:HALF, :]], axis=0)
    there = swapped[:, 0:1]
    gap = here - there
    centre = 0.5 * (here + there)
    spread = (around + swapped[:, 64:65] + 256.0 * gap * gap) / 1024.0
    scale = lax.rsqrt(spread + EPSILON)
    for k in range(FS):
        at = slice(k * 128, (k + 1) * 128)
        v = (cvals[:, at] - centre) * scale * cgain_ref[:, at] + cshift_ref[:, at]
        raw[:, k * 256 + 128 : (k + 1) * 256] = (v / (1.0 + jnp.exp(-v))).astype(BF16)

    for i in range(1, FS):
        feat_wait(1, fs_of(i))
    for k in range(FS):
        raw[0:HALF, k * 256 : k * 256 + 128] = fatt[k, other_half]
        raw[HALF:TOK, k * 256 : k * 256 + 128] = fatt[k, own_half]

    serve_b(gather_out, 4, 0, 4)

    def part_copy(n):
        return pltpu.make_async_remote_copy(
            src_ref=part_out.at[n],
            dst_ref=part_in.at[n],
            send_sem=part_sent,
            recv_sem=part_recv.at[n],
            device_id={"tp": partner},
            device_id_type=MESH,
        )

    for n in range(D // CHUNK):
        weights = wout[n * CHUNK : (n + 1) * CHUNK, :]
        product = lax.dot_general(raw[...], weights, NT, preferred_element_type=F32)
        part_out[n] = product[0:HALF].astype(BF16)
        part_copy(n).start()
        part[n] = product[HALF:TOK]
    for n in range(D // CHUNK):
        part_copy(n).wait_recv()
        out_ref[:, n * CHUNK : (n + 1) * CHUNK] = (part[n] + part_in[n].astype(F32)).astype(BF16)

    def drain(ref, sent):
        pltpu.make_async_remote_copy(
            src_ref=ref,
            dst_ref=ref,
            send_sem=sent,
            recv_sem=stat_recv.at[0],
            device_id={"tp": partner},
            device_id_type=MESH,
        ).wait_send()

    drain(part_out, part_sent)
    stat_copy.wait_send()
    drain(sconv.at[1:FS], conv_sent)
    drain(satt.at[1:FS], att_sent)

    @pl.when(has_low)
    def _():
        drain(kvg.at[:, 0:144], halo_sent[0])

    @pl.when(has_high)
    def _():
        drain(kvg.at[:, 144:288], halo_sent[1])

    drain(tok.at[0:3], tok_sent)
    end_gather(gather_in)
    end_gather(gather_out)


def local(
    tokens,
    norm_gain,
    w_query,
    w_key,
    w_value,
    w_conv_in,
    w_conv_gate,
    sink_logit,
    conv_taps,
    conv_bias,
    channel_gain,
    channel_shift,
    w_attn_out,
    w_conv_out,
):
    vmem = pl.BlockSpec(memory_space=pltpu.VMEM)
    anywhere = pl.BlockSpec(memory_space=pl.ANY)
    dma = pltpu.SemaphoreType.DMA
    args = (
        tokens,
        norm_gain.reshape(1, -1),
        w_query,
        w_key,
        w_value,
        w_conv_in,
        w_conv_gate,
        sink_logit.reshape(1, -1),
        conv_taps,
        conv_bias.reshape(1, -1),
        channel_gain.reshape(1, -1),
        channel_shift.reshape(1, -1),
        w_attn_out.T,
        w_conv_out.T,
    )
    return pl.pallas_call(
        kernel,
        out_shape=jax.ShapeDtypeStruct((HALF, D), BF16),
        in_specs=[anywhere] * len(args),
        out_specs=vmem,
        scratch_shapes=[pltpu.VMEM(a.shape, a.dtype) for a in args]
        + [
            pltpu.VMEM((FS, TOK, D), BF16),
            pltpu.VMEM((D, 512), BF16),
            pltpu.VMEM((D, 1024), BF16),
            pltpu.VMEM((TOK, 128), F32),
            pltpu.VMEM((TOK, 128), F32),
            pltpu.VMEM((FS, 2, TOK, 128), BF16),
            pltpu.VMEM((FS, 288, 128), BF16),
            pltpu.VMEM((FS, 288, 128), F32),
            pltpu.VMEM((FS, 144, 128), BF16),
            pltpu.VMEM((FS, 144, 128), BF16),
            pltpu.VMEM((FS, TOK, 128), BF16),
            pltpu.VMEM((FS, TOK, 128), BF16),
            pltpu.VMEM((FS, TOK, 128), BF16),
            pltpu.VMEM((FS, TOK, 128), BF16),
            pltpu.VMEM((TOK, 1024), BF16),
            pltpu.VMEM((TOK, 512), F32),
            pltpu.VMEM((TOK, 128), F32),
            pltpu.VMEM((TOK, 128), F32),
            pltpu.VMEM((D // CHUNK, HALF, CHUNK), F32),
            pltpu.VMEM((D // CHUNK, HALF, CHUNK), BF16),
            pltpu.VMEM((D // CHUNK, HALF, CHUNK), BF16),
            dma((15,)),
            dma((RING,)),
            dma((RING, 4)),
            dma((RING,)),
            dma((RING, 4)),
            dma((FS, 2, 2)),
            dma((FS, 2)),
            dma((2, FS)),
            dma((1,)),
            dma((D // CHUNK,)),
            dma((9,)),
        ],
        compiler_params=pltpu.CompilerParams(
            collective_id=0, has_side_effects=True, vmem_limit_bytes=32 * 1024 * 1024
        ),
        name="fused",
    )(*(pltpu.with_memory_space_constraint(a, pltpu.HBM) for a in args))


def solution(mesh):
    in_specs = (
        P(("fs", "sp"), None),
        P(),
        P("sp", "tp"),
        P("sp", "tp"),
        P("sp", "tp"),
        P("sp", "tp"),
        P("sp", "tp"),
        P("tp"),
        P(None, "tp"),
        P("tp"),
        P("tp"),
        P("tp"),
        P(None, "sp"),
        P(None, "sp"),
    )
    out_specs = P(("fs", "sp", "tp"), None)
    return jax.shard_map(local, mesh=mesh, in_specs=in_specs, out_specs=out_specs, check_vma=False)
```
